32 devices in a mesh: sp: 8 (over z, y), tp: 4 (over x, core).
Axes of the slice: x: 2, y: 2, z: 4, core: 2. Of those that a mesh axis runs over, the one named last changes fastest.
Arguments:
- memory_queries: bfloat16 [4096, 1024], P('sp', 'tp'), may hold values from -8 to 8
- memory_keys: bfloat16 [4096, 1024], P('sp', 'tp'), may hold values from -8 to 8
- memory_values: bfloat16 [4096, 1024], P('sp', 'tp'), may hold values from -6 to 6
- input_gate_logits: float32 [8, 4096], P('tp', 'sp'), may hold values from -64 to 160
- forget_gate_logits: float32 [8, 4096], P('tp', 'sp'), may hold values from -0.1 to 20
- extra_log_decay: float32 [8, 4096], P('tp', 'sp'), may hold values from -1.4 to 0
- residual: bfloat16 [4096, 2048], P(('sp', 'tp')), may hold values from -6 to 6
- cell_output_weight: bfloat16 [1024, 2048], P('tp', 'sp'), may hold values from -0.1875 to 0.1875
- expert_norm_gain: float32 [2048], replicated, may hold values from 0.1 to 1.9
- expert_gate_weight: bfloat16 [8, 2048, 3584], P('sp', None, 'tp'), may hold values from -0.125 to 0.125
- expert_up_weight: bfloat16 [8, 2048, 3584], P('sp', None, 'tp'), may hold values from -0.125 to 0.125
- expert_down_weight: bfloat16 [8, 3584, 2048], P('sp', 'tp'), may hold values from -0.09375 to 0.09375
- routed_expert_index: int32 [4096, 2], P('sp'), may hold values from 0 to 7, as said below
- routed_expert_weight: float32 [4096, 2], P(('sp', 'tp')), may hold values from 0.1 to 1
Outputs:
- layer_out: bfloat16 [4096, 2048], P(('sp', 'tp'))
The draws below stay inside these ranges and needn't reach their ends.
Inputs may be any that keep to these rules, and one draw needn't show every extreme that they name: `routed_expert_index`: each row names 2 different experts. In each aligned block of 128 rows (the rows of one device after the cell) no expert is named more than 40 times, and one expert is named exactly 40 times in every block.
All inputs are finite; a program needn't handle non-finite values.
Results may differ from the reference program's by a relative error of at most 0.013.
Values may be sent and summed in bfloat16 or wider, within the bound.
A program may use at most 128 MiB of HBM per device.

```python
import math
import jax
import jax.numpy as jnp
from jax import lax

D = 2048
RECURRENT_LANES = 8
DH = 128
FF = 3584
TOPK = 2
TOK_DEV = 512
TEXT_LENGTH = 4096
ROWS = 128
HD = 1024
EXPERTS = 8
CAP = 40
EXPERT_ROWS = 1280
N_TP = 4


def shared_direction(key):
    return jnp.clip(jax.random.normal(jax.random.fold_in(key, 3), (RECURRENT_LANES * DH,), jnp.float32), -4.0, 4.0)


def query_like(key, salt_id):
    offset = 0.95
    dims_all = (TEXT_LENGTH, RECURRENT_LANES * DH)
    jitter = jnp.clip(jax.random.normal(jax.random.fold_in(key, salt_id), dims_all, jnp.float32), -4.0, 4.0)
    return jitter + offset * shared_direction(key)[None, :]


def draw_memory_queries(key, part):
    return query_like(key, 5).astype(jnp.bfloat16)


def draw_memory_keys(key, part):
    return query_like(key, 6).astype(jnp.bfloat16)


def draw_input_gate_logits(key, part):
    dims_all = (RECURRENT_LANES, TEXT_LENGTH)
    return 2.5 * jnp.clip(jax.random.normal(jax.random.fold_in(key, 8), dims_all, jnp.float32), -4.0, 4.0)


def draw_forget_gate_logits(key, part):
    ranking = jax.random.permutation(jax.random.fold_in(key, 12), RECURRENT_LANES)
    quick_count = RECURRENT_LANES // 2
    center = jnp.where(ranking < quick_count, math.log(40.0), math.log(TEXT_LENGTH) + 1.5).astype(jnp.float32)
    device_shift = jax.random.uniform(jax.random.fold_in(key, 13), (TEXT_LENGTH // TOK_DEV,), jnp.float32, -0.7, 0.7)
    device_shift = jnp.repeat(device_shift, TOK_DEV)
    jitter = jnp.clip(jax.random.normal(jax.random.fold_in(key, 14), (RECURRENT_LANES, TEXT_LENGTH), jnp.float32), -3.0, 3.0)
    return center[:, None] + device_shift[None, :] + jitter


def draw_extra_log_decay(key, part):
    surge_offset = jax.random.randint(jax.random.fold_in(key, 15), (RECURRENT_LANES, 3, 1), 0, TEXT_LENGTH)
    element_levels = jax.random.uniform(jax.random.fold_in(key, 16), (RECURRENT_LANES, 3, 1), jnp.float32, -0.69, -0.22)
    seat_locations = jnp.arange(TEXT_LENGTH)[None, None, :]
    return jnp.sum(jnp.where(seat_locations == surge_offset, element_levels, 0.0), axis=1)


def draw_routed_expert_index(key, part):
    specialist_capacity = EXPERTS * CAP
    assigned = ROWS * TOPK
    specialist_table = jnp.arange(specialist_capacity) // CAP
    favour_increment = jax.random.randint(jax.random.fold_in(key, 21), (EXPERTS,), 0, 3) * 4096
    chosen_specialists = jax.random.randint(jax.random.fold_in(key, 22), (), 0, EXPERTS)
    additional_reward = favour_increment[specialist_table] + jnp.where(specialist_table == chosen_specialists, 16384, 0)

    def one_block(address_tile_range):
        dispatch_affinity = jax.random.randint(jax.random.fold_in(address_tile_range, 1), (specialist_capacity,), 0, 4096) + additional_reward
        ranked = dispatch_affinity * specialist_capacity + jnp.arange(specialist_capacity)
        picked = lax.top_k(ranked, assigned)[1]
        names = jnp.sort(specialist_table[picked]).reshape(TOPK, ROWS).T
        turn = jax.random.randint(jax.random.fold_in(address_tile_range, 2), (ROWS, 1), 0, TOPK)
        names = jnp.take_along_axis(names, (jnp.arange(TOPK)[None, :] + turn) % TOPK, axis=1)
        return names[jax.random.permutation(jax.random.fold_in(address_tile_range, 3), ROWS)]
    block_keys = jax.random.split(jax.random.fold_in(key, 23), TEXT_LENGTH // ROWS)
    return jax.vmap(one_block)(block_keys).reshape(TEXT_LENGTH, TOPK).astype(jnp.int32)


def level_of(own_key, shape, cuts, smallest, largest):
    level = 1.0
    for axis_at, shards_of in cuts:
        draws = jax.random.uniform(jax.random.fold_in(jax.random.fold_in(own_key, 6), axis_at), (shards_of,), jnp.float32, smallest / len(cuts), largest / len(cuts))
        level = level * jnp.repeat(jnp.exp(draws), shape[axis_at] // shards_of).reshape((-1,) + (1,) * (len(shape) - 1 - axis_at))
    return level


def gaussian(rng, dims, scale, bound, shards=(), held_as=jnp.bfloat16):
    drawn = jax.random.normal(rng, dims, jnp.float32) * scale
    if len(shards) > 0:
        drawn = level_of(rng, dims, shards, -0.22, 0.18) * drawn
    return jnp.clip(drawn, min=-bound, max=bound).astype(held_as)


def setup_inputs(seed: int = 0) -> dict:
    key_list = jax.random.split(jax.random.key(seed), 15)
    return {
        "memory_queries": draw_memory_queries(jax.random.fold_in(key_list[14], 71), 0),
        "memory_keys": draw_memory_keys(jax.random.fold_in(key_list[14], 71), 0),
        "memory_values": gaussian(key_list[2], (TEXT_LENGTH, HD), 1.0, 6.0, ((0, 8), (1, 4))),
        "input_gate_logits": draw_input_gate_logits(jax.random.fold_in(key_list[14], 71), 0),
        "forget_gate_logits": draw_forget_gate_logits(jax.random.fold_in(key_list[14], 71), 0),
        "extra_log_decay": draw_extra_log_decay(jax.random.fold_in(key_list[14], 71), 0),
        "residual": gaussian(key_list[6], (TEXT_LENGTH, D), 1.0, 6.0, ((0, 32),)),
        "cell_output_weight": gaussian(key_list[7], (HD, D), HD ** -0.5, 0.1875, ((0, 4), (1, 8))),
        "expert_norm_gain": jnp.clip(1.0 + 0.18 * jax.random.normal(key_list[8], (D,), jnp.float32), 0.1, 1.9),
        "expert_gate_weight": gaussian(key_list[9], (EXPERTS, D, FF), D ** -0.5, 0.125, ((0, 8), (2, 4))),
        "expert_up_weight": gaussian(key_list[10], (EXPERTS, D, FF), D ** -0.5, 0.125, ((0, 8), (2, 4))),
        "expert_down_weight": gaussian(key_list[11], (EXPERTS, FF, D), FF ** -0.5, 0.09375, ((0, 8), (1, 4))),
        "routed_expert_index": draw_routed_expert_index(jax.random.fold_in(key_list[14], 71), 0),
        "routed_expert_weight": jnp.clip(0.1 + 0.9 * jax.random.uniform(key_list[13], (TEXT_LENGTH, TOPK), jnp.float32) ** level_of(key_list[13], (TEXT_LENGTH, TOPK), ((0, 32),), -0.2, 0.2), 0.1, 1.0),
    }


highest = lax.Precision.HIGHEST
lowest = -1e+30
epsilon = 1e-06

def block_pass(memory, inputs):
    state_mat, state_norm, state_max = memory
    queries, keys_blk, values_blk, gate_in, forget_log_value = inputs
    length = gate_in.shape[-1]
    running = jnp.cumsum(forget_log_value, axis=-1)
    causal = jnp.arange(length)[:, None] >= jnp.arange(length)[None, :]
    exponent = running[:, :, None] - running[:, None, :] + gate_in[:, None, :]
    exponent = jnp.where(causal[None], exponent, -jnp.inf)
    carried = running + state_max[:, None]
    row_max = jnp.maximum(carried, lax.optimization_barrier(jnp.max(exponent, axis=-1)))
    decays = jnp.exp(exponent - row_max[:, :, None])
    carry_scale = jnp.exp(carried - row_max)
    dispatch_affinity = jnp.einsum('htk,hsk->hts', queries, keys_blk, precision=highest) * decays
    numerator = carry_scale[:, :, None] * jnp.einsum('hvk,htk->htv', state_mat, queries, precision=highest)
    numerator = numerator + jnp.einsum('hts,hsv->htv', dispatch_affinity, values_blk, precision=highest)
    denominator = carry_scale * jnp.einsum('hk,htk->ht', state_norm, queries, precision=highest) + lax.optimization_barrier(jnp.sum(dispatch_affinity, axis=-1))
    final_log = running[:, -1]
    log_prev = final_log + state_max
    log_keep = final_log[:, None] - running + gate_in
    new_max = jnp.maximum(log_prev, lax.optimization_barrier(jnp.max(log_keep, axis=-1)))
    prev_scale = jnp.exp(log_prev - new_max)
    retain = jnp.exp(log_keep - new_max[:, None])
    new_mat = prev_scale[:, None, None] * state_mat + jnp.einsum('hsv,hsk->hvk', retain[:, :, None] * values_blk, keys_blk, precision=highest)
    new_norm = prev_scale[:, None] * state_norm + jnp.einsum('hs,hsk->hk', retain, keys_blk, precision=highest)
    output = numerator / jnp.maximum(jnp.abs(denominator), jnp.exp(-row_max))[:, :, None]
    return ((new_mat, new_norm, new_max), output)

def heads_first(tensor):
    return jnp.transpose(tensor.astype(jnp.float32).reshape(TEXT_LENGTH, RECURRENT_LANES, DH), (1, 0, 2))

def reference(memory_queries, memory_keys, memory_values, input_gate_logits, forget_gate_logits, extra_log_decay, residual, cell_output_weight, expert_norm_gain, expert_gate_weight, expert_up_weight, expert_down_weight, routed_expert_index, routed_expert_weight):
    block_size = min(TOK_DEV, 256)
    block_count = TEXT_LENGTH // block_size

    def split_blocks(tensor):
        return jnp.moveaxis(tensor.reshape((RECURRENT_LANES, block_count, block_size) + tensor.shape[2:]), 1, 0)
    queries = heads_first(memory_queries) * DH ** (-0.5)
    forget_log_value = jax.nn.log_sigmoid(forget_gate_logits) + extra_log_decay
    start_state = (jnp.zeros((RECURRENT_LANES, DH, DH), jnp.float32), jnp.zeros((RECURRENT_LANES, DH), jnp.float32), jnp.full((RECURRENT_LANES,), lowest, jnp.float32))
    members = (queries, heads_first(memory_keys), heads_first(memory_values), input_gate_logits, forget_log_value)
    end_state, outputs = lax.scan(block_pass, start_state, tuple((split_blocks(member) for member in members)))
    hidden = jnp.moveaxis(outputs, 0, 1).reshape(RECURRENT_LANES, TEXT_LENGTH, DH).astype(jnp.bfloat16)
    flat_hidden = jnp.transpose(hidden, (1, 0, 2)).reshape(TEXT_LENGTH, HD)
    quarter = HD // N_TP
    projected = jnp.zeros((TEXT_LENGTH, D), jnp.float32)
    for owner_idx in range(N_TP):
        low_col = owner_idx * quarter
        group_term = jnp.dot(flat_hidden[:, low_col:low_col + quarter], cell_output_weight[low_col:low_col + quarter], preferred_element_type=jnp.float32)
        projected = projected + lax.optimization_barrier(group_term.astype(jnp.bfloat16)).astype(jnp.float32)
    mixed_rows = (residual.astype(jnp.float32) + projected).astype(jnp.bfloat16)
    mixed_wide = mixed_rows.astype(jnp.float32)
    norm_scale = lax.rsqrt(lax.optimization_barrier(jnp.mean(mixed_wide * mixed_wide, axis=-1, keepdims=True)) + epsilon)
    normed = (mixed_wide * norm_scale * expert_norm_gain).astype(jnp.bfloat16)
    normed_pad = jnp.concatenate([normed, jnp.zeros((1, D), jnp.bfloat16)], axis=0)
    hidden_part = FF // N_TP

    def one_expert(running_sum, expert):
        matched = routed_expert_index == expert
        weight_tok = jnp.concatenate([lax.optimization_barrier(jnp.sum(jnp.where(matched, routed_expert_weight, 0.0), axis=1)), jnp.zeros((1,), jnp.float32)])
        picked = jnp.nonzero(jnp.any(matched, axis=1), size=EXPERT_ROWS, fill_value=TEXT_LENGTH)[0]
        rows_in = normed_pad[picked]
        gate_all = expert_gate_weight[expert]
        up_all = expert_up_weight[expert]
        down_all = expert_down_weight[expert]
        result = jnp.zeros((EXPERT_ROWS, D), jnp.float32)
        for owner_idx in range(N_TP):
            low_col = owner_idx * hidden_part
            gate_pre = jnp.dot(rows_in, gate_all[:, low_col:low_col + hidden_part], preferred_element_type=jnp.float32)
            up_pre = jnp.dot(rows_in, up_all[:, low_col:low_col + hidden_part], preferred_element_type=jnp.float32)
            hidden_act = (jax.nn.silu(gate_pre) * up_pre).astype(jnp.bfloat16)
            group_term = jnp.dot(hidden_act, down_all[low_col:low_col + hidden_part], preferred_element_type=jnp.float32)
            result = result + lax.optimization_barrier(group_term.astype(jnp.bfloat16)).astype(jnp.float32)
        returned = lax.optimization_barrier(result.astype(jnp.bfloat16)).astype(jnp.float32)
        return (running_sum.at[picked].add(returned * weight_tok[picked][:, None], mode='drop'), None)
    routed, _ = lax.scan(one_expert, jnp.zeros((TEXT_LENGTH, D), jnp.float32), jnp.arange(EXPERTS, dtype=jnp.int32))
    return (mixed_wide + routed).astype(jnp.bfloat16)
```

```python
import functools
import jax
import jax.numpy as jnp
from jax import lax
from jax.experimental import pallas as pl
from jax.experimental.pallas import tpu as pltpu
from jax.sharding import PartitionSpec as P

highest = lax.Precision.HIGHEST
lowest = -1e30
epsilon = 1e-06


def places():
    sp, tp = lax.axis_index("sp"), lax.axis_index("tp")
    n = lax.axis_size("sp")
    return sp, tp, n, tp + 1 - 2 * (tp % 2), (tp + 2) % 4


def greet(devices):
    barrier = pltpu.get_barrier_semaphore()
    for device in devices:
        pl.semaphore_signal(
            barrier, inc=1, device_id=device, device_id_type=pl.DeviceIdType.MESH
        )
    pl.semaphore_wait(barrier, len(devices))


def remote(src, dst, send, recv, device):
    return pltpu.make_async_remote_copy(
        src_ref=src,
        dst_ref=dst,
        send_sem=send,
        recv_sem=recv,
        device_id=device,
        device_id_type=pl.DeviceIdType.MESH,
    )


def far_first(n):
    return sorted(range(1, n), key=lambda k: abs(2 * k - n))


def flip(place, k, bits):
    out = place
    for b in range(bits):
        step = 1 << b
        out = out + ((k // step) % 2) * step * (1 - 2 * ((place // step) % 2))
    return out


def experts_kernel(
    x_ref, gate_hbm, up_hbm, down_hbm, share_ref, mixed_ref, out_ref,
    gate_up, down, arrive, part, near, sent, far, result, home,
    weight_sems, direct_s, direct_r, across_s, across_r, side_s, side_r, relay_s, relay_r,
    near_s, near_r, far_s, far_r, home_s, home_r,
):
    sp, tp, n, p, q = places()
    bits = n.bit_length() - 1
    half = n // 2
    hidden = down.shape[0]
    width = x_ref.shape[2]
    rows = x_ref.shape[1]
    pulls = [
        pltpu.make_async_copy(gate_hbm.at[0], gate_up.at[:, pl.ds(0, hidden)], weight_sems.at[0]),
        pltpu.make_async_copy(up_hbm.at[0], gate_up.at[:, pl.ds(hidden, hidden)], weight_sems.at[1]),
        pltpu.make_async_copy(down_hbm.at[0], down, weight_sems.at[2]),
    ]
    for pull in pulls:
        pull.start()
    greet([(flip(sp, k, bits), tp) for k in range(1, n)] + [(sp, p), (sp, q)])

    def turn(i):
        late = i // half
        return (1 - late) * (half + i) + late * (n - 1 - i)

    def direct(i):
        k = turn(i)
        other = flip(sp, k, bits)
        return remote(
            x_ref.at[other], arrive.at[sp, tp], direct_s.at[i], direct_r.at[i], (other, tp)
        )

    def across(i, src):
        s = flip(sp, turn(i), bits)
        return remote(src(s), arrive.at[s, tp], across_s.at[i], across_r.at[i], (sp, q))

    def side(i, src):
        s = flip(sp, turn(i), bits)
        return remote(src(s), arrive.at[s, tp], side_s.at[i], side_r.at[i], (sp, p))

    def landed(s):
        return arrive.at[s, tp]

    def mine(s):
        return x_ref.at[s]

    def relay(i):
        s = flip(sp, turn(i), bits)
        return remote(
            arrive.at[s, q], arrive.at[s, q], relay_s.at[i], relay_r.at[i], (sp, p)
        )

    def near_far(i):
        s = flip(sp, turn(i), bits)
        return remote(
            part.at[s, (p + 2) % 4], near.at[0, i], near_s.at[0, i], near_r.at[0, i], (sp, p)
        )

    def near_own(i):
        s = flip(sp, turn(i), bits)
        return remote(part.at[s, p], near.at[1, i], near_s.at[1, i], near_r.at[1, i], (sp, p))

    def crossing(i):
        return remote(sent.at[i], far.at[i], far_s.at[i], far_r.at[i], (sp, q))

    def homeward(i):
        other = flip(sp, turn(i), bits)
        return remote(result.at[i], home.at[sp], home_s.at[i], home_r.at[i], (other, tp))

    @pl.loop(0, n - 1)
    def _(i):
        direct(i).start()

    across(n - 1, mine).start()
    side(n - 1, mine).start()
    arrive[sp, tp] = x_ref[sp]
    for pull in pulls:
        pull.wait()

    @pl.loop(0, n + 4)
    def _(i):
        @pl.when(i < n - 1)
        def _():
            direct(i).wait_recv()
            across(i, landed).start()
            side(i, landed).start()

        @pl.when((i >= 1) & (i <= n))
        def _():
            across(i - 1, landed).wait_recv()
            relay(i - 1).start()

        @pl.when((i >= 2) & (i <= n + 1))
        def _():
            j = i - 2
            s = flip(sp, turn(j), bits)
            side(j, landed).wait_recv()
            relay(j).wait_recv()
            pre = jnp.dot(
                arrive[s].reshape(4 * rows, width), gate_up[...],
                preferred_element_type=jnp.float32,
            )
            gate = pre[:, :hidden]
            act = (gate / (1.0 + jnp.exp(-gate)) * pre[:, hidden:]).astype(jnp.bfloat16)
            out = jnp.dot(act, down[...], preferred_element_type=jnp.float32)
            part[s] = out.astype(jnp.bfloat16).reshape(4, rows, width)
            near_far(j).start()
            near_own(j).start()

        @pl.when((i >= 3) & (i <= n + 2))
        def _():
            j = i - 3
            s = flip(sp, turn(j), bits)
            near_far(j).wait_recv()
            total = part[s, q].astype(jnp.float32) + near[0, j].astype(jnp.float32)
            sent[j] = total.astype(jnp.bfloat16)
            crossing(j).start()

        @pl.when(i >= 4)
        def _():
            j = i - 4
            s = flip(sp, turn(j), bits)
            near_own(j).wait_recv()
            crossing(j).wait_recv()
            total = part[s, tp].astype(jnp.float32) + near[1, j].astype(jnp.float32)
            result[j] = (total + far[j].astype(jnp.float32)).astype(jnp.bfloat16)

            @pl.when(j < n - 1)
            def _():
                homeward(j).start()

    home[sp] = result[n - 1]

    @pl.loop(0, n - 1)
    def _(i):
        homeward(i).wait()
        direct(i).wait_send()

    @pl.loop(0, n)
    def _(i):
        across(i, landed).wait_send()
        side(i, landed).wait_send()
        relay(i).wait_send()
        near_far(i).wait_send()
        near_own(i).wait_send()
        crossing(i).wait_send()

    share = share_ref[...]
    coarse = share.astype(jnp.bfloat16)
    fine = (share - coarse.astype(jnp.float32)).astype(jnp.bfloat16)
    back = home[...].reshape(n * rows, width)
    routed = jnp.dot(coarse, back, preferred_element_type=jnp.float32)
    routed = routed + jnp.dot(fine, back, preferred_element_type=jnp.float32)
    out_ref[...] = (mixed_ref[...].astype(jnp.float32) + routed).astype(jnp.bfloat16)


def experts_stage(x, gate, up, down, share, mixed):
    n, rows, width = x.shape
    hidden = down.shape[1]
    block = (n, rows, width)
    vmem = pl.BlockSpec(memory_space=pltpu.VMEM)
    hbm = pl.BlockSpec(memory_space=pl.ANY)
    dma = pltpu.SemaphoreType.DMA
    return pl.pallas_call(
        experts_kernel,
        out_shape=jax.ShapeDtypeStruct(mixed.shape, mixed.dtype),
        in_specs=[vmem, hbm, hbm, hbm, vmem, vmem],
        out_specs=vmem,
        scratch_shapes=[
            pltpu.VMEM((width, 2 * hidden), x.dtype),
            pltpu.VMEM((hidden, width), x.dtype),
            pltpu.VMEM((n, 4, rows, width), x.dtype),
            pltpu.VMEM((n, 4, rows, width), x.dtype),
            pltpu.VMEM((2,) + block, x.dtype),
            pltpu.VMEM(block, x.dtype),
            pltpu.VMEM(block, x.dtype),
            pltpu.VMEM(block, x.dtype),
            pltpu.VMEM(block, x.dtype),
            dma((3,)),
        ]
        + [dma((n,))] * 8
        + [dma((2, n))] * 2
        + [dma((n,))] * 4,
        compiler_params=pltpu.CompilerParams(
            collective_id=1, has_side_effects=True, vmem_limit_bytes=60 * 2**20
        ),
    )(x, gate, up, down, share, mixed)


def collect_kernel(back, x_ref, out_ref, near, sent, far, result, send_sems, recv_sems):
    sp, tp, n, p, q = places()
    chunks = x_ref.shape[1]
    offsets = far_first(n) + [0]
    peers = [((sp + k) % n, tp) for k in offsets[:-1]] if back else []
    greet(peers + [(sp, p), (sp, q)])

    def at(k):
        return (sp + offsets[k]) % n if back else k

    near_far, near_own, crossing, homeward = [], [], [], []
    for k in range(chunks):
        copy = remote(
            x_ref.at[(p + 2) % 4, at(k)], near.at[0, k],
            send_sems.at[0, k], recv_sems.at[0, k], (sp, p),
        )
        copy.start()
        near_far.append(copy)
    for k in range(chunks):
        copy = remote(
            x_ref.at[p, at(k)], near.at[1, k], send_sems.at[1, k], recv_sems.at[1, k], (sp, p)
        )
        copy.start()
        near_own.append(copy)
    for k in range(chunks):
        near_far[k].wait_recv()
        total = x_ref[q, at(k)].astype(jnp.float32) + near[0, k].astype(jnp.float32)
        sent[k] = total.astype(jnp.bfloat16)
        copy = remote(sent.at[k], far.at[k], send_sems.at[2, k], recv_sems.at[2, k], (sp, q))
        copy.start()
        crossing.append(copy)
    for k in range(chunks):
        near_own[k].wait_recv()
        crossing[k].wait_recv()
        total = x_ref[tp, at(k)].astype(jnp.float32) + near[1, k].astype(jnp.float32)
        total = (total + far[k].astype(jnp.float32)).astype(jnp.bfloat16)
        if not back:
            out_ref[k] = total
        elif k == chunks - 1:
            out_ref[sp] = total
        else:
            result[k] = total
            copy = remote(
                result.at[k], out_ref.at[sp], send_sems.at[3, k], recv_sems.at[3, k], peers[k]
            )
            copy.start()
            homeward.append(copy)
    for copy in homeward:
        copy.wait()
    for copy in near_far + near_own + crossing:
        copy.wait_send()


def collect(x, back):
    _, n, rows, width = x.shape
    block = (n, rows, width)
    return pl.pallas_call(
        functools.partial(collect_kernel, back),
        out_shape=jax.ShapeDtypeStruct(block, x.dtype),
        in_specs=[pl.BlockSpec(memory_space=pltpu.VMEM)],
        out_specs=pl.BlockSpec(memory_space=pltpu.VMEM),
        scratch_shapes=[
            pltpu.VMEM((2,) + block, x.dtype),
            pltpu.VMEM(block, x.dtype),
            pltpu.VMEM(block, x.dtype),
            pltpu.VMEM(block if back else (1, 16, 128), x.dtype),
            pltpu.SemaphoreType.DMA((4, n)),
            pltpu.SemaphoreType.DMA((4, n)),
        ],
        compiler_params=pltpu.CompilerParams(
            collective_id=2 if back else 3, has_side_effects=True, vmem_limit_bytes=58 * 2**20
        ),
    )(x)


def spread_kernel(x_ref, out_ref, send_sems, recv_sems):
    sp, tp, n, _, _ = places()
    half = n // 2
    twin = sp + 1 - 2 * (sp % 2)
    peers = [((sp + 2 * k) % n, tp) for k in range(1, half)]
    greet(peers + [(twin, tp)])
    first, second = [None], []
    for k in range(1, half):
        copy = remote(
            x_ref, out_ref.at[sp], send_sems.at[0, k], recv_sems.at[0, k], peers[k - 1]
        )
        copy.start()
        first.append(copy)
    for k in range(half):
        s = (sp - 2 * k + n) % n
        if k == 0:
            src = x_ref
        else:
            first[k].wait_recv()
            src = out_ref.at[s]
        copy = remote(src, out_ref.at[s], send_sems.at[1, k], recv_sems.at[1, k], (twin, tp))
        copy.start()
        second.append(copy)
        if k == 0:
            out_ref[sp] = x_ref[...]
    for copy in second:
        copy.wait()
    for copy in first[1:]:
        copy.wait_send()


def spread(x):
    n = lax.axis_size("sp")
    half = n // 2
    return pl.pallas_call(
        spread_kernel,
        out_shape=jax.ShapeDtypeStruct((n,) + x.shape, x.dtype),
        in_specs=[pl.BlockSpec(memory_space=pltpu.VMEM)],
        out_specs=pl.BlockSpec(memory_space=pltpu.VMEM),
        scratch_shapes=[pltpu.SemaphoreType.DMA((2, half)), pltpu.SemaphoreType.DMA((2, half))],
        compiler_params=pltpu.CompilerParams(
            collective_id=4, has_side_effects=True, vmem_limit_bytes=58 * 2**20
        ),
    )(x)


def carried_in(x):
    log_sum, mat, norm, top = x
    heads, dim, _ = mat.shape
    n, place = lax.axis_size("sp"), lax.axis_index("sp")
    scalars = jnp.broadcast_to(jnp.concatenate([log_sum, top])[:, None], (2 * heads, dim))
    packed = jnp.concatenate([mat.reshape(heads * dim, dim), norm, scalars], axis=0)
    used = packed.shape[0]
    packed = jnp.pad(packed, ((0, -used % 8), (0, 0)))
    everything = spread(packed)
    mats = everything[:, : heads * dim].reshape(n, heads, dim, dim)
    norms = everything[:, heads * dim : heads * dim + heads]
    logs = everything[:, heads * dim + heads : heads * dim + 2 * heads, 0]
    tops = everything[:, heads * dim + 2 * heads : heads * dim + 3 * heads, 0]
    index = jnp.arange(n)
    reached = index < place
    between = (index[None, :] > index[:, None]) & reached[None, :]
    decay = jnp.sum(jnp.where(between[:, :, None], logs[None], 0.0), axis=1)
    level = jnp.where(reached[:, None], tops + decay, lowest)
    prior_max = jnp.max(level, axis=0)
    scale = jnp.where(reached[:, None], jnp.exp(level - prior_max), 0.0)
    prior_mat = jnp.sum(scale[:, :, None, None] * mats, axis=0)
    prior_norm = jnp.sum(scale[:, :, None] * norms, axis=0)
    return prior_mat, prior_norm, prior_max


def block_pass(memory, inputs):
    state_mat, state_norm, state_max = memory
    queries, keys_blk, values_blk, gate_in, forget_log_value = inputs
    length = gate_in.shape[-1]
    running = jnp.cumsum(forget_log_value, axis=-1)
    causal = jnp.arange(length)[:, None] >= jnp.arange(length)[None, :]
    exponent = running[:, :, None] - running[:, None, :] + gate_in[:, None, :]
    exponent = jnp.where(causal[None], exponent, -jnp.inf)
    carried = running + state_max[:, None]
    row_max = jnp.maximum(carried, jnp.max(exponent, axis=-1))
    decays = jnp.exp(exponent - row_max[:, :, None])
    carry_scale = jnp.exp(carried - row_max)
    dispatch_affinity = jnp.einsum("htk,hsk->hts", queries, keys_blk, precision=highest) * decays
    numerator = carry_scale[:, :, None] * jnp.einsum(
        "hvk,htk->htv", state_mat, queries, precision=highest
    )
    numerator = numerator + jnp.einsum(
        "hts,hsv->htv", dispatch_affinity, values_blk, precision=highest
    )
    denominator = carry_scale * jnp.einsum(
        "hk,htk->ht", state_norm, queries, precision=highest
    ) + jnp.sum(dispatch_affinity, axis=-1)
    final_log = running[:, -1]
    log_prev = final_log + state_max
    log_keep = final_log[:, None] - running + gate_in
    new_max = jnp.maximum(log_prev, jnp.max(log_keep, axis=-1))
    prev_scale = jnp.exp(log_prev - new_max)
    retain = jnp.exp(log_keep - new_max[:, None])
    new_mat = prev_scale[:, None, None] * state_mat + jnp.einsum(
        "hsv,hsk->hvk", retain[:, :, None] * values_blk, keys_blk, precision=highest
    )
    new_norm = prev_scale[:, None] * state_norm + jnp.einsum(
        "hs,hsk->hk", retain, keys_blk, precision=highest
    )
    return ((new_mat, new_norm, new_max), (numerator, denominator, row_max))


def matrix_memory_step(
    memory_queries,
    memory_keys,
    memory_values,
    input_gate_logits,
    forget_gate_logits,
    extra_log_decay,
):
    tokens_here, channels = memory_queries.shape
    heads_here = input_gate_logits.shape[0]
    head_dim = channels // heads_here

    def heads_first(tensor):
        pieces = [
            tensor[:, head * head_dim : (head + 1) * head_dim] for head in range(heads_here)
        ]
        return jnp.stack(pieces).astype(jnp.float32)

    queries = heads_first(memory_queries) * head_dim ** (-0.5)
    forget_log_value = jax.nn.log_sigmoid(forget_gate_logits) + extra_log_decay
    block_size = min(tokens_here, 256)
    block_count = tokens_here // block_size

    def split_blocks(tensor):
        return jnp.moveaxis(
            tensor.reshape((heads_here, block_count, block_size) + tensor.shape[2:]), 1, 0
        )

    def join_blocks(tensor):
        return jnp.moveaxis(tensor, 0, 1).reshape((heads_here, tokens_here) + tensor.shape[3:])

    empty_state = (
        jnp.zeros((heads_here, head_dim, head_dim), jnp.float32),
        jnp.zeros((heads_here, head_dim), jnp.float32),
        jnp.full((heads_here,), lowest, jnp.float32),
    )
    members = (
        queries,
        heads_first(memory_keys),
        heads_first(memory_values),
        input_gate_logits,
        forget_log_value,
    )
    end_state, pieces = lax.scan(
        block_pass, empty_state, tuple((split_blocks(member) for member in members))
    )
    numerator, denominator, row_max = (join_blocks(member) for member in pieces)
    running = jnp.cumsum(forget_log_value, axis=-1)
    prior_mat, prior_norm, prior_max = carried_in((running[:, -1],) + tuple(end_state))
    reached = running + prior_max[:, None]
    joined = jnp.maximum(row_max, reached)
    local_scale = jnp.exp(row_max - joined)
    carry_scale = jnp.exp(reached - joined)
    numerator = local_scale[:, :, None] * numerator + carry_scale[:, :, None] * jnp.einsum(
        "hvk,htk->htv", prior_mat, queries, precision=highest
    )
    denominator = local_scale * denominator + carry_scale * jnp.einsum(
        "hk,htk->ht", prior_norm, queries, precision=highest
    )
    guarded = jnp.maximum(jnp.abs(denominator), jnp.exp(-joined))
    return ((numerator / guarded[:, :, None]).astype(jnp.bfloat16), heads_here, head_dim)


def slot_index(ids, experts, capacity):
    flat_ids = ids.reshape(-1)
    matches = (flat_ids[:, None] == jnp.arange(experts, dtype=jnp.int32)[None, :]).astype(jnp.int32)
    before = jnp.cumsum(matches, axis=0) - matches
    return flat_ids * capacity + jnp.sum(before * matches, axis=1)


def local(
    memory_queries,
    memory_keys,
    memory_values,
    input_gate_logits,
    forget_gate_logits,
    extra_log_decay,
    residual,
    cell_output_weight,
    expert_norm_gain,
    expert_gate_weight,
    expert_up_weight,
    expert_down_weight,
    routed_expert_index,
    routed_expert_weight,
):
    hidden, heads_here, head_dim = matrix_memory_step(
        memory_queries,
        memory_keys,
        memory_values,
        input_gate_logits,
        forget_gate_logits,
        extra_log_decay,
    )
    weight_piece = lax.all_gather(cell_output_weight, "sp", axis=1, tiled=True)
    shaped = weight_piece.reshape(heads_here, head_dim, weight_piece.shape[1])
    partial_rows = jnp.einsum(
        "htd,hdc->tc", hidden, shaped, preferred_element_type=jnp.float32
    ).astype(jnp.bfloat16)
    row_count, model_width = residual.shape
    projected = collect(partial_rows.reshape(4, 4, row_count // 4, model_width), False)
    projected = projected.reshape(row_count, model_width).astype(jnp.float32)
    mixed_rows = (residual.astype(jnp.float32) + projected).astype(jnp.bfloat16)
    mixed_wide = mixed_rows.astype(jnp.float32)
    norm_scale = lax.rsqrt(jnp.mean(mixed_wide * mixed_wide, axis=-1, keepdims=True) + epsilon)
    normed = (mixed_wide * norm_scale * expert_norm_gain).astype(jnp.bfloat16)
    sp_size = lax.axis_size("sp")
    top_count = routed_expert_index.shape[1]
    experts = sp_size * expert_gate_weight.shape[0]
    assigned = row_count * top_count
    capacity = max(2, assigned * 5 // (4 * experts))
    own_ids = lax.dynamic_slice_in_dim(
        routed_expert_index, lax.axis_index("tp") * row_count, row_count, 0
    )
    own_slots = slot_index(own_ids, experts, capacity)
    slots = own_slots.reshape(row_count, top_count)
    at_slot = slots[:, :, None] == jnp.arange(experts * capacity, dtype=jnp.int32)
    chosen = jnp.any(at_slot, axis=1).astype(jnp.bfloat16)
    outgoing = lax.dot_general(
        chosen, normed, (((0,), (0,)), ((), ())), preferred_element_type=jnp.float32
    ).astype(jnp.bfloat16)
    padded = -(-capacity // 8) * 8
    outgoing = jnp.pad(
        outgoing.reshape(experts, capacity, model_width), ((0, 0), (0, padded - capacity), (0, 0))
    )
    share = jnp.sum(jnp.where(at_slot, routed_expert_weight[:, :, None], 0.0), axis=1)
    share = jnp.pad(
        share.reshape(row_count, experts, capacity), ((0, 0), (0, 0), (0, padded - capacity))
    )
    return experts_stage(
        outgoing,
        expert_gate_weight,
        expert_up_weight,
        expert_down_weight,
        share.reshape(row_count, experts * padded),
        mixed_rows,
    )


def solution(mesh):
    return jax.shard_map(
        local,
        mesh=mesh,
        in_specs=(
            P("sp", "tp"),
            P("sp", "tp"),
            P("sp", "tp"),
            P("tp", "sp"),
            P("tp", "sp"),
            P("tp", "sp"),
            P(("sp", "tp"), None),
            P("tp", "sp"),
            P(),
            P("sp", None, "tp"),
            P("sp", None, "tp"),
            P("sp", "tp", None),
            P("sp", None),
            P(("sp", "tp"), None),
        ),
        out_specs=P(("sp", "tp"), None),
        check_vma=False,
    )
```

```python
import functools
import jax
import jax.numpy as jnp
from jax import lax
from jax.experimental import pallas as pl
from jax.experimental.pallas import tpu as pltpu
from jax.sharding import PartitionSpec as P

highest = lax.Precision.HIGHEST
lowest = -1e30
epsilon = 1e-06


def places():
    sp, tp = lax.axis_index("sp"), lax.axis_index("tp")
    n = lax.axis_size("sp")
    return sp, tp, n, tp + 1 - 2 * (tp % 2), (tp + 2) % 4


def greet(devices):
    barrier = pltpu.get_barrier_semaphore()
    for device in devices:
        pl.semaphore_signal(
            barrier, inc=1, device_id=device, device_id_type=pl.DeviceIdType.MESH
        )
    pl.semaphore_wait(barrier, len(devices))


def remote(src, dst, send, recv, device):
    return pltpu.make_async_remote_copy(
        src_ref=src,
        dst_ref=dst,
        send_sem=send,
        recv_sem=recv,
        device_id=device,
        device_id_type=pl.DeviceIdType.MESH,
    )


def flip(place, k, bits):
    out = place
    for b in range(bits):
        step = 1 << b
        out = out + ((k // step) % 2) * step * (1 - 2 * ((place // step) % 2))
    return out


def narrow(x):
    coarse = x.astype(jnp.bfloat16)
    return coarse, (x - coarse.astype(jnp.float32)).astype(jnp.bfloat16)


def matmul(a, b):
    return jnp.dot(a, b, preferred_element_type=jnp.float32)


def matmul_t(a, b):
    return lax.dot_general(a, b, (((0,), (0,)), ((), ())), preferred_element_type=jnp.float32)


def matmul_nt(a, b):
    return lax.dot_general(a, b, (((1,), (1,)), ((), ())), preferred_element_type=jnp.float32)


def stack_rows(pieces, length):
    used = sum(piece.shape[0] for piece in pieces)
    return jnp.concatenate(list(pieces) + [jnp.zeros((-used % 8, length), jnp.float32)], axis=0)


def running_sum(x):
    rows, length = x.shape
    parts, rest = [], x
    for _ in range(3):
        part = rest.astype(jnp.bfloat16).astype(jnp.float32)
        parts.append(part)
        rest = rest - part
    stacked = stack_rows(parts, length).astype(jnp.bfloat16)
    at = lax.broadcasted_iota(jnp.int32, (length, length), 0)
    to = lax.broadcasted_iota(jnp.int32, (length, length), 1)
    sums = matmul(stacked, jnp.where(at <= to, 1.0, 0.0).astype(jnp.bfloat16))
    return sums[:rows] + sums[rows : 2 * rows] + sums[2 * rows : 3 * rows]


def running_max(x):
    length = x.shape[1]
    lane = lax.broadcasted_iota(jnp.int32, x.shape, 1)
    step = 1
    while step < length:
        x = jnp.maximum(x, jnp.where(lane >= step, pltpu.roll(x, step, 1), lowest))
        step *= 2
    return x


def slot_tables(ids, weights, experts, capacity, padded):
    rows = ids.shape[1]
    names = lax.broadcasted_iota(jnp.int32, (experts, rows), 0)
    hits = [ids[j : j + 1] == names for j in range(ids.shape[0])]
    named = sum(jnp.where(hit, 1.0, 0.0) for hit in hits)
    at = lax.broadcasted_iota(jnp.int32, (rows, rows), 0)
    to = lax.broadcasted_iota(jnp.int32, (rows, rows), 1)
    before = matmul(named.astype(jnp.bfloat16), jnp.where(at < to, 1.0, 0.0).astype(jnp.bfloat16))
    slot = lax.broadcasted_iota(jnp.int32, (experts * padded, rows), 0)
    chosen, share = 0.0, 0.0
    for j, hit in enumerate(hits):
        rank = jnp.sum(jnp.where(hit, before, 0.0), axis=0, keepdims=True)
        here = (ids[j : j + 1] * padded + rank.astype(jnp.int32)) == slot
        chosen = chosen + jnp.where(here, 1.0, 0.0)
        share = share + jnp.where(here, weights[j : j + 1], 0.0)
    return chosen.astype(jnp.bfloat16), share


def cell_kernel(
    experts, capacity, padded,
    q_ref, k_ref, v_ref, in_ref, forget_ref, extra_ref, res_ref, w_ref, gain_ref, ids_ref, wts_ref,
    out_ref, mixed_ref, share_ref,
    mine, mats, tiny_mine, tiny, pieces, pairs, hid, partial, near, sent, far,
    mat_s, mat_r, tiny_s, tiny_r, piece_s, piece_r, near_s, near_r, far_s, far_r,
):
    sp, tp, n, p, q = places()
    bits = n.bit_length() - 1
    length, channels = q_ref.shape
    heads = in_ref.shape[0]
    dim = channels // heads
    rows, width = res_ref.shape
    columns = w_ref.shape[1]
    evens = list(range(n - 2, 0, -2))
    evens = evens[len(evens) // 2 :][:1] + evens[: len(evens) // 2] + evens[len(evens) // 2 + 1 :]

    def at(k):
        return flip(sp, k, bits)

    def mat_copy(k):
        src = mine if k < 2 else (mine if k % 2 == 0 else mats.at[at(k - 1)])
        slot = sp if k % 2 == 0 or k == 1 else at(k - 1)
        to = at(1) if k % 2 else at(k)
        return remote(src, mats.at[slot], mat_s.at[k], mat_r.at[k], (to, tp))

    def tiny_copy(k):
        src = tiny_mine if k % 2 == 0 or k == 1 else tiny.at[at(k - 1)]
        slot = sp if k % 2 == 0 or k == 1 else at(k - 1)
        to = at(1) if k % 2 else at(k)
        return remote(src, tiny.at[slot], tiny_s.at[k], tiny_r.at[k], (to, tp))

    def piece_copy(k):
        src = w_ref if k % 2 == 0 or k == 1 else pieces.at[at(k - 1)]
        slot = sp if k % 2 == 0 or k == 1 else at(k - 1)
        to = at(1) if k % 2 else at(k)
        return remote(src, pieces.at[slot], piece_s.at[k], piece_r.at[k], (to, tp))

    greet([(at(k), tp) for k in [1] + evens] + [(sp, p), (sp, q)])
    piece_copy(1).start()
    piece_copy(evens[0]).start()

    logits = forget_ref[...]
    log_forget = (
        jnp.minimum(logits, 0.0) - jnp.log1p(jnp.exp(-jnp.abs(logits))) + extra_ref[...]
    )
    total = running_sum(log_forget)
    level = in_ref[...] - total
    peak = jnp.max(level, axis=1, keepdims=True)
    retain = jnp.exp(level - peak)
    retain_columns = jnp.transpose(stack_rows([retain], length))
    for h in range(heads):
        lanes = slice(h * dim, (h + 1) * dim)
        kept = narrow(v_ref[:, lanes].astype(jnp.float32) * retain_columns[:, h : h + 1])
        mat = matmul_t(k_ref[:, lanes], kept[0]) + matmul_t(k_ref[:, lanes], kept[1])
        mine[lanes, :] = mat.astype(jnp.bfloat16)
    coarse, fine = narrow(retain)
    sums = matmul(
        stack_rows([coarse.astype(jnp.float32), fine.astype(jnp.float32)], length).astype(jnp.bfloat16),
        k_ref[...],
    )
    norms = [
        sums[h : h + 1, h * dim : (h + 1) * dim]
        + sums[heads + h : heads + h + 1, h * dim : (h + 1) * dim]
        for h in range(heads)
    ]
    last = total[:, length - 1 : length]
    tiny_mine[...] = stack_rows(
        norms + [jnp.broadcast_to(last, (heads, dim)), jnp.broadcast_to(last + peak, (heads, dim))], dim
    )
    for k in evens + [1]:
        tiny_copy(k).start()
        mat_copy(k).start()
    for k in evens[1:]:
        piece_copy(k).start()
    mats[sp] = mine[...]
    tiny[sp] = tiny_mine[...]
    pieces[sp] = w_ref[...]

    top = running_max(level)
    top_columns = jnp.transpose(stack_rows([top], length))
    block = min(length, 256)
    for h in range(heads):
        lanes = slice(h * dim, (h + 1) * dim)
        widened = jnp.concatenate(
            [v_ref[:, lanes], jnp.ones((length, dim), jnp.bfloat16)], axis=1
        )
        for first in range(0, length, block):
            end = first + block
            scores = matmul_nt(q_ref[first:end, lanes], k_ref[:end, lanes])
            gap = level[h : h + 1, :end] - top_columns[first:end, h : h + 1]
            t = lax.broadcasted_iota(jnp.int32, (block, end), 0) + first
            s = lax.broadcasted_iota(jnp.int32, (block, end), 1)
            scores = scores * jnp.exp(jnp.where(s <= t, gap, lowest))
            coarse, fine = narrow(scores)
            pairs[h, first:end] = matmul(coarse, widened[:end]) + matmul(fine, widened[:end])

    chosen, share = slot_tables(ids_ref[...], wts_ref[...], experts, capacity, padded)
    share_ref[...] = share

    for k in evens:
        tiny_copy(k).wait_recv()
        tiny_copy(k + 1).start()
        mat_copy(k).wait_recv()
        mat_copy(k + 1).start()
    piece_copy(evens[0]).wait_recv()
    piece_copy(evens[0] + 1).start()
    for k in [1] + [k + 1 for k in evens]:
        tiny_copy(k).wait_recv()
        mat_copy(k).wait_recv()

    decay = jnp.zeros((heads, dim), jnp.float32)
    levels, flags = [None] * n, [None] * n
    for s in reversed(range(n)):
        flags[s] = jnp.where(s < sp, 1.0, 0.0)
        levels[s] = flags[s] * (tiny[s, 2 * heads : 3 * heads] + decay) + (1.0 - flags[s]) * lowest
        decay = decay + flags[s] * tiny[s, heads : 2 * heads]
    prior_top = functools.reduce(jnp.maximum, levels)
    scales = [jnp.exp(levels[s] - prior_top) * flags[s] for s in range(n)]
    prior_norm = sum(scales[s] * tiny[s, :heads] for s in range(n))
    norm_columns = jnp.transpose(stack_rows([prior_norm], dim))
    reach = jnp.broadcast_to(prior_top[:, :1], (heads, length))
    joined = jnp.maximum(top, reach)
    factors = jnp.transpose(
        stack_rows(
            [
                jnp.exp(top - joined),
                jnp.exp(reach - joined),
                jnp.exp(-(total + joined)) * dim**0.5,
            ],
            length,
        )
    )
    for h in range(heads):
        lanes = slice(h * dim, (h + 1) * dim)
        prior = sum(
            scales[s][h : h + 1] * mats[s, lanes, :].astype(jnp.float32) for s in range(n)
        )
        prior = jnp.concatenate(
            [prior, jnp.broadcast_to(norm_columns[:, h : h + 1], (dim, dim))], axis=1
        )
        coarse, fine = narrow(prior)
        carried = matmul(q_ref[:, lanes], coarse) + matmul(q_ref[:, lanes], fine)
        both = pairs[h] * factors[:, h : h + 1]
        both = both + carried * factors[:, heads + h : heads + h + 1]
        guard = jnp.maximum(
            jnp.abs(both[:, dim:]), factors[:, 2 * heads + h : 2 * heads + h + 1]
        )
        hid[:, lanes] = (both[:, :dim] / guard).astype(jnp.bfloat16)

    group = max(1, 256 // columns)
    chunk = group * columns
    count = width // chunk

    def pass_on(k):
        piece_copy(k).wait_recv()
        piece_copy(k + 1).start()

    def near_far(i):
        return remote(
            partial.at[i, (p + 2) % 4], near.at[0, i], near_s.at[0, i], near_r.at[0, i], (sp, p)
        )

    def near_own(i):
        return remote(partial.at[i, p], near.at[1, i], near_s.at[1, i], near_r.at[1, i], (sp, p))

    def crossing(i):
        return remote(sent.at[i], far.at[i], far_s.at[i], far_r.at[i], (sp, q))

    def cross(i):
        near_far(i).wait_recv()
        both = partial[i, q].astype(jnp.float32) + near[0, i].astype(jnp.float32)
        sent[i] = both.astype(jnp.bfloat16)
        crossing(i).start()

    if group == 1:
        order = [0, 1, evens[0], evens[0] + 1] + evens[1:] + [k + 1 for k in evens[1:]]
        spots = [at(k) for k in order]
    else:
        order = spots = list(range(count))
        for k in evens[1:]:
            pass_on(k)
        for k in [1] + [k + 1 for k in evens]:
            piece_copy(k).wait_recv()
    for i, k in enumerate(order):
        if group > 1:
            piece = jnp.concatenate([pieces[i * group + j] for j in range(group)], axis=1)
        else:
            if k % 2:
                piece_copy(k).wait_recv()
            elif k in evens[1:]:
                pass_on(k)
            piece = pieces[spots[i]]
        made = matmul(hid[...], piece).astype(jnp.bfloat16)
        partial[i] = made.reshape(length // rows, rows, chunk)
        near_far(i).start()
        near_own(i).start()
        if i:
            cross(i - 1)
    cross(count - 1)

    squares = jnp.zeros((rows, 1), jnp.float32)
    for i in range(count):
        near_own(i).wait_recv()
        crossing(i).wait_recv()
        where = pl.ds(pl.multiple_of(spots[i] * chunk, chunk), chunk)
        both = partial[i, tp].astype(jnp.float32) + near[1, i].astype(jnp.float32)
        both = both + far[i].astype(jnp.float32)
        mixed = (res_ref[:, where].astype(jnp.float32) + both).astype(jnp.bfloat16)
        mixed_ref[:, where] = mixed
        wide = mixed.astype(jnp.float32)
        squares = squares + jnp.sum(wide * wide, axis=1, keepdims=True)
    scale = lax.rsqrt(squares / width + epsilon)
    span = min(width, 512)
    for first in range(0, width, span):
        wide = mixed_ref[:, first : first + span].astype(jnp.float32)
        normed = (wide * scale * gain_ref[:, first : first + span]).astype(jnp.bfloat16)
        picked = matmul(chosen, normed).astype(jnp.bfloat16)
        out_ref[:, :, first : first + span] = picked.reshape(experts, padded, span)

    for k in range(1, n):
        tiny_copy(k).wait_send()
        mat_copy(k).wait_send()
        piece_copy(k).wait_send()
    for i in range(count):
        near_far(i).wait_send()
        near_own(i).wait_send()
        crossing(i).wait_send()


def cell_stage(capacity, q, k, v, gate_in, forget, extra, residual, weight, gain, ids, wts):
    n = lax.axis_size("sp")
    length, channels = q.shape
    heads = gate_in.shape[0]
    dim = channels // heads
    rows, width = residual.shape
    columns = weight.shape[1]
    chunk = max(1, 256 // columns) * columns
    count = width // chunk
    padded = -(-capacity // 8) * 8
    vmem = pl.BlockSpec(memory_space=pltpu.VMEM)
    dma = pltpu.SemaphoreType.DMA
    kind = residual.dtype
    return pl.pallas_call(
        functools.partial(cell_kernel, n, capacity, padded),
        out_shape=(
            jax.ShapeDtypeStruct((n, padded, width), kind),
            jax.ShapeDtypeStruct((rows, width), kind),
            jax.ShapeDtypeStruct((n * padded, rows), jnp.float32),
        ),
        in_specs=[vmem] * 11,
        out_specs=(vmem,) * 3,
        scratch_shapes=[
            pltpu.VMEM((channels, dim), kind),
            pltpu.VMEM((n, channels, dim), kind),
            pltpu.VMEM((8, dim), jnp.float32),
            pltpu.VMEM((n, 8, dim), jnp.float32),
            pltpu.VMEM((n, channels, columns), kind),
            pltpu.VMEM((heads, length, 2 * dim), jnp.float32),
            pltpu.VMEM((length, channels), kind),
            pltpu.VMEM((count, length // rows, rows, chunk), kind),
            pltpu.VMEM((2, count, rows, chunk), kind),
            pltpu.VMEM((count, rows, chunk), kind),
            pltpu.VMEM((count, rows, chunk), kind),
        ]
        + [dma((n,))] * 6
        + [dma((2, count))] * 2
        + [dma((count,))] * 2,
        compiler_params=pltpu.CompilerParams(
            collective_id=2, has_side_effects=True, vmem_limit_bytes=58 * 2**20
        ),
    )(q, k, v, gate_in, forget, extra, residual, weight, gain, ids, wts)


def experts_kernel(
    x_ref, gate_hbm, up_hbm, down_hbm, share_ref, mixed_ref, out_ref,
    gate_up, down, arrive, part, near, sent, far, result, home,
    weight_sems, direct_s, direct_r, across_s, across_r, side_s, side_r, relay_s, relay_r,
    near_s, near_r, far_s, far_r, home_s, home_r,
):
    sp, tp, n, p, q = places()
    bits = n.bit_length() - 1
    half = n // 2
    hidden = down.shape[0]
    width = x_ref.shape[2]
    rows = x_ref.shape[1]
    pulls = [
        pltpu.make_async_copy(gate_hbm.at[0], gate_up.at[:, pl.ds(0, hidden)], weight_sems.at[0]),
        pltpu.make_async_copy(up_hbm.at[0], gate_up.at[:, pl.ds(hidden, hidden)], weight_sems.at[1]),
        pltpu.make_async_copy(down_hbm.at[0], down, weight_sems.at[2]),
    ]
    for pull in pulls:
        pull.start()
    greet([(flip(sp, k, bits), tp) for k in range(1, n)] + [(sp, p), (sp, q)])

    def turn(i):
        late = i // half
        return (1 - late) * (half + i) + late * (n - 1 - i)

    def direct(i):
        k = turn(i)
        other = flip(sp, k, bits)
        return remote(
            x_ref.at[other], arrive.at[sp, tp], direct_s.at[i], direct_r.at[i], (other, tp)
        )

    def across(i, src):
        s = flip(sp, turn(i), bits)
        return remote(src(s), arrive.at[s, tp], across_s.at[i], across_r.at[i], (sp, q))

    def side(i, src):
        s = flip(sp, turn(i), bits)
        return remote(src(s), arrive.at[s, tp], side_s.at[i], side_r.at[i], (sp, p))

    def landed(s):
        return arrive.at[s, tp]

    def mine(s):
        return x_ref.at[s]

    def relay(i):
        s = flip(sp, turn(i), bits)
        return remote(
            arrive.at[s, q], arrive.at[s, q], relay_s.at[i], relay_r.at[i], (sp, p)
        )

    def near_far(i):
        s = flip(sp, turn(i), bits)
        return remote(
            part.at[s, (p + 2) % 4], near.at[0, i], near_s.at[0, i], near_r.at[0, i], (sp, p)
        )

    def near_own(i):
        s = flip(sp, turn(i), bits)
        return remote(part.at[s, p], near.at[1, i], near_s.at[1, i], near_r.at[1, i], (sp, p))

    def crossing(i):
        return remote(sent.at[i], far.at[i], far_s.at[i], far_r.at[i], (sp, q))

    def homeward(i):
        other = flip(sp, turn(i), bits)
        return remote(result.at[i], home.at[sp], home_s.at[i], home_r.at[i], (other, tp))

    @pl.loop(0, n - 1)
    def _(i):
        direct(i).start()

    across(n - 1, mine).start()
    side(n - 1, mine).start()
    arrive[sp, tp] = x_ref[sp]
    for pull in pulls:
        pull.wait()

    @pl.loop(0, n + 4)
    def _(i):
        @pl.when(i < n - 1)
        def _():
            direct(i).wait_recv()
            across(i, landed).start()
            side(i, landed).start()

        @pl.when((i >= 1) & (i <= n))
        def _():
            across(i - 1, landed).wait_recv()
            relay(i - 1).start()

        @pl.when((i >= 2) & (i <= n + 1))
        def _():
            j = i - 2
            s = flip(sp, turn(j), bits)
            side(j, landed).wait_recv()
            relay(j).wait_recv()
            pre = jnp.dot(
                arrive[s].reshape(4 * rows, width), gate_up[...],
                preferred_element_type=jnp.float32,
            )
            gate = pre[:, :hidden]
            act = (gate / (1.0 + jnp.exp(-gate)) * pre[:, hidden:]).astype(jnp.bfloat16)
            out = jnp.dot(act, down[...], preferred_element_type=jnp.float32)
            part[s] = out.astype(jnp.bfloat16).reshape(4, rows, width)
            near_far(j).start()
            near_own(j).start()

        @pl.when((i >= 3) & (i <= n + 2))
        def _():
            j = i - 3
            s = flip(sp, turn(j), bits)
            near_far(j).wait_recv()
            total = part[s, q].astype(jnp.float32) + near[0, j].astype(jnp.float32)
            sent[j] = total.astype(jnp.bfloat16)
            crossing(j).start()

        @pl.when(i >= 4)
        def _():
            j = i - 4
            s = flip(sp, turn(j), bits)
            near_own(j).wait_recv()
            crossing(j).wait_recv()
            total = part[s, tp].astype(jnp.float32) + near[1, j].astype(jnp.float32)
            result[j] = (total + far[j].astype(jnp.float32)).astype(jnp.bfloat16)

            @pl.when(j < n - 1)
            def _():
                homeward(j).start()

    home[sp] = result[n - 1]

    @pl.loop(0, n - 1)
    def _(i):
        homeward(i).wait()
        direct(i).wait_send()

    @pl.loop(0, n)
    def _(i):
        across(i, landed).wait_send()
        side(i, landed).wait_send()
        relay(i).wait_send()
        near_far(i).wait_send()
        near_own(i).wait_send()
        crossing(i).wait_send()

    share = share_ref[...]
    coarse, fine = narrow(share)
    back = home[...].reshape(n * rows, width)
    routed = matmul_t(coarse, back) + matmul_t(fine, back)
    out_ref[...] = (mixed_ref[...].astype(jnp.float32) + routed).astype(jnp.bfloat16)


def experts_stage(x, gate, up, down, share, mixed):
    n, rows, width = x.shape
    hidden = down.shape[1]
    block = (n, rows, width)
    vmem = pl.BlockSpec(memory_space=pltpu.VMEM)
    hbm = pl.BlockSpec(memory_space=pl.ANY)
    dma = pltpu.SemaphoreType.DMA
    return pl.pallas_call(
        experts_kernel,
        out_shape=jax.ShapeDtypeStruct(mixed.shape, mixed.dtype),
        in_specs=[vmem, hbm, hbm, hbm, vmem, vmem],
        out_specs=vmem,
        scratch_shapes=[
            pltpu.VMEM((width, 2 * hidden), x.dtype),
            pltpu.VMEM((hidden, width), x.dtype),
            pltpu.VMEM((n, 4, rows, width), x.dtype),
            pltpu.VMEM((n, 4, rows, width), x.dtype),
            pltpu.VMEM((2,) + block, x.dtype),
            pltpu.VMEM(block, x.dtype),
            pltpu.VMEM(block, x.dtype),
            pltpu.VMEM(block, x.dtype),
            pltpu.VMEM(block, x.dtype),
            dma((3,)),
        ]
        + [dma((n,))] * 8
        + [dma((2, n))] * 2
        + [dma((n,))] * 4,
        compiler_params=pltpu.CompilerParams(
            collective_id=1, has_side_effects=True, vmem_limit_bytes=60 * 2**20
        ),
    )(x, gate, up, down, share, mixed)


def local(
    memory_queries,
    memory_keys,
    memory_values,
    input_gate_logits,
    forget_gate_logits,
    extra_log_decay,
    residual,
    cell_output_weight,
    expert_norm_gain,
    expert_gate_weight,
    expert_up_weight,
    expert_down_weight,
    routed_expert_index,
    routed_expert_weight,
):
    row_count = residual.shape[0]
    experts = lax.axis_size("sp") * expert_gate_weight.shape[0]
    assigned = row_count * routed_expert_index.shape[1]
    capacity = max(2, assigned * 5 // (4 * experts))
    own_ids = lax.dynamic_slice_in_dim(
        routed_expert_index, lax.axis_index("tp") * row_count, row_count, 0
    )
    outgoing, mixed, share = cell_stage(
        capacity,
        memory_queries,
        memory_keys,
        memory_values,
        input_gate_logits,
        forget_gate_logits,
        extra_log_decay,
        residual,
        cell_output_weight,
        expert_norm_gain[None, :],
        own_ids.T,
        routed_expert_weight.T,
    )
    return experts_stage(
        outgoing, expert_gate_weight, expert_up_weight, expert_down_weight, share, mixed
    )


def solution(mesh):
    return jax.shard_map(
        local,
        mesh=mesh,
        in_specs=(
            P("sp", "tp"),
            P("sp", "tp"),
            P("sp", "tp"),
            P("tp", "sp"),
            P("tp", "sp"),
            P("tp", "sp"),
            P(("sp", "tp"), None),
            P("tp", "sp"),
            P(),
            P("sp", None, "tp"),
            P("sp", None, "tp"),
            P("sp", "tp", None),
            P("sp", None),
            P(("sp", "tp"), None),
        ),
        out_specs=P(("sp", "tp"), None),
        check_vma=False,
    )
```

```python
import functools
import jax
import jax.numpy as jnp
from jax import lax
from jax.experimental import pallas as pl
from jax.experimental.pallas import tpu as pltpu
from jax.sharding import PartitionSpec as P

highest = lax.Precision.HIGHEST
lowest = -1e30
epsilon = 1e-06


def places():
    sp, tp = lax.axis_index("sp"), lax.axis_index("tp")
    n = lax.axis_size("sp")
    return sp, tp, n, tp + 1 - 2 * (tp % 2), (tp + 2) % 4


def announce(devices):
    barrier = pltpu.get_barrier_semaphore()
    for device in devices:
        pl.semaphore_signal(
            barrier, inc=1, device_id=device, device_id_type=pl.DeviceIdType.MESH
        )
    return len(devices)


def remote(src, dst, send, recv, device):
    return pltpu.make_async_remote_copy(
        src_ref=src,
        dst_ref=dst,
        send_sem=send,
        recv_sem=recv,
        device_id=device,
        device_id_type=pl.DeviceIdType.MESH,
    )


def flip(place, k, bits):
    out = place
    for b in range(bits):
        step = 1 << b
        out = out + ((k // step) % 2) * step * (1 - 2 * ((place // step) % 2))
    return out


def narrow(x):
    coarse = x.astype(jnp.bfloat16)
    return coarse, (x - coarse.astype(jnp.float32)).astype(jnp.bfloat16)


def matmul(a, b):
    return jnp.dot(a, b, preferred_element_type=jnp.float32)


def matmul_t(a, b):
    return lax.dot_general(a, b, (((0,), (0,)), ((), ())), preferred_element_type=jnp.float32)


def matmul_nt(a, b):
    return lax.dot_general(a, b, (((1,), (1,)), ((), ())), preferred_element_type=jnp.float32)


def stack_rows(pieces, length):
    used = sum(piece.shape[0] for piece in pieces)
    return jnp.concatenate(list(pieces) + [jnp.zeros((-used % 8, length), jnp.float32)], axis=0)


def running_sum(x):
    rows, length = x.shape
    parts, rest = [], x
    for _ in range(3):
        part = rest.astype(jnp.bfloat16).astype(jnp.float32)
        parts.append(part)
        rest = rest - part
    stacked = stack_rows(parts, length).astype(jnp.bfloat16)
    at = lax.broadcasted_iota(jnp.int32, (length, length), 0)
    to = lax.broadcasted_iota(jnp.int32, (length, length), 1)
    sums = matmul(stacked, jnp.where(at <= to, 1.0, 0.0).astype(jnp.bfloat16))
    return sums[:rows] + sums[rows : 2 * rows] + sums[2 * rows : 3 * rows]


def running_max(x):
    length = x.shape[1]
    lane = lax.broadcasted_iota(jnp.int32, x.shape, 1)
    step = 1
    while step < length:
        x = jnp.maximum(x, jnp.where(lane >= step, pltpu.roll(x, step, 1), lowest))
        step *= 2
    return x


def slot_tables(ids, weights, experts, capacity, padded):
    rows = ids.shape[1]
    names = lax.broadcasted_iota(jnp.int32, (experts, rows), 0)
    hits = [ids[j : j + 1] == names for j in range(ids.shape[0])]
    named = sum(jnp.where(hit, 1.0, 0.0) for hit in hits)
    at = lax.broadcasted_iota(jnp.int32, (rows, rows), 0)
    to = lax.broadcasted_iota(jnp.int32, (rows, rows), 1)
    before = matmul(named.astype(jnp.bfloat16), jnp.where(at < to, 1.0, 0.0).astype(jnp.bfloat16))
    slot = lax.broadcasted_iota(jnp.int32, (experts * padded, rows), 0)
    chosen, share = 0.0, 0.0
    for j, hit in enumerate(hits):
        rank = jnp.sum(jnp.where(hit, before, 0.0), axis=0, keepdims=True)
        here = (ids[j : j + 1] * padded + rank.astype(jnp.int32)) == slot
        chosen = chosen + jnp.where(here, 1.0, 0.0)
        share = share + jnp.where(here, weights[j : j + 1], 0.0)
    return chosen.astype(jnp.bfloat16), share


def layer_kernel(
    capacity, padded,
    q_hbm, k_ref, v_ref, in_ref, forget_ref, extra_ref, res_hbm, w_hbm, gain_ref, ids_ref, wts_ref,
    gate_hbm, up_hbm, down_hbm, out_ref,
    q_ref, res_ref, mine, mats, tiny_mine, tiny, pieces, pairs, hid, partial, near, sent, far,
    x_ref, mixed_ref, share_ref, gate_up, down, arrive, part, close, paid, other_half, result,
    home, routed,
    load_sems, mat_s, mat_r, tiny_s, tiny_r, piece_s, piece_r, near_s, near_r, far_s, far_r,
    direct_s, direct_r, across_s, across_r, side_s, side_r, relay_s, relay_r,
    close_s, close_r, paid_s, paid_r, home_s, home_r,
):
    sp, tp, n, p, q = places()
    bits = n.bit_length() - 1
    length, channels = k_ref.shape
    heads = in_ref.shape[0]
    dim = channels // heads
    rows, width = out_ref.shape
    columns = pieces.shape[2]
    hidden = down.shape[0]
    experts = n
    count_greeted = announce([(flip(sp, k, bits), tp) for k in range(1, n)] + [(sp, p), (sp, q)])
    loads = [
        pltpu.make_async_copy(w_hbm, pieces.at[sp], load_sems.at[0]),
        pltpu.make_async_copy(q_hbm, q_ref, load_sems.at[1]),
        pltpu.make_async_copy(res_hbm, res_ref, load_sems.at[2]),
        pltpu.make_async_copy(gate_hbm.at[0], gate_up.at[:, pl.ds(0, hidden)], load_sems.at[3]),
        pltpu.make_async_copy(up_hbm.at[0], gate_up.at[:, pl.ds(hidden, hidden)], load_sems.at[4]),
        pltpu.make_async_copy(down_hbm.at[0], down, load_sems.at[5]),
    ]
    for load in loads:
        load.start()
    evens = list(range(2, n, 2))

    def at(k):
        return flip(sp, k, bits)

    def mat_copy(k):
        src = mine if k < 2 else (mine if k % 2 == 0 else mats.at[at(k - 1)])
        slot = sp if k % 2 == 0 or k == 1 else at(k - 1)
        to = at(1) if k % 2 else at(k)
        return remote(src, mats.at[slot], mat_s.at[k], mat_r.at[k], (to, tp))

    def tiny_copy(k):
        src = tiny_mine if k % 2 == 0 or k == 1 else tiny.at[at(k - 1)]
        slot = sp if k % 2 == 0 or k == 1 else at(k - 1)
        to = at(1) if k % 2 else at(k)
        return remote(src, tiny.at[slot], tiny_s.at[k], tiny_r.at[k], (to, tp))

    def piece_copy(k):
        slot = sp if k % 2 == 0 or k == 1 else at(k - 1)
        src = pieces.at[slot]
        to = at(1) if k % 2 else at(k)
        return remote(src, pieces.at[slot], piece_s.at[k], piece_r.at[k], (to, tp))

    logits = forget_ref[...]
    log_forget = (
        jnp.minimum(logits, 0.0) - jnp.log1p(jnp.exp(-jnp.abs(logits))) + extra_ref[...]
    )
    total = running_sum(log_forget)
    level = in_ref[...] - total
    peak = jnp.max(level, axis=1, keepdims=True)
    retain = jnp.exp(level - peak)
    retain_columns = jnp.transpose(stack_rows([retain], length))
    for h in range(heads):
        lanes = slice(h * dim, (h + 1) * dim)
        kept = narrow(v_ref[:, lanes].astype(jnp.float32) * retain_columns[:, h : h + 1])
        mat = matmul_t(k_ref[:, lanes], kept[0]) + matmul_t(k_ref[:, lanes], kept[1])
        mine[lanes, :] = mat.astype(jnp.bfloat16)
    coarse, fine = narrow(retain)
    sums = matmul(
        stack_rows([coarse.astype(jnp.float32), fine.astype(jnp.float32)], length).astype(jnp.bfloat16),
        k_ref[...],
    )
    norms = [
        sums[h : h + 1, h * dim : (h + 1) * dim]
        + sums[heads + h : heads + h + 1, h * dim : (h + 1) * dim]
        for h in range(heads)
    ]
    last = total[:, length - 1 : length]
    tiny_mine[...] = stack_rows(
        norms + [jnp.broadcast_to(last, (heads, dim)), jnp.broadcast_to(last + peak, (heads, dim))], dim
    )
    pl.semaphore_wait(pltpu.get_barrier_semaphore(), count_greeted)
    for k in evens + [1]:
        tiny_copy(k).start()
        mat_copy(k).start()
    loads[0].wait()
    for k in [1] + evens:
        piece_copy(k).start()
    mats[sp] = mine[...]
    tiny[sp] = tiny_mine[...]
    loads[1].wait()

    top = running_max(level)
    top_columns = jnp.transpose(stack_rows([top], length))
    block = min(length, 256)
    for h in range(heads):
        lanes = slice(h * dim, (h + 1) * dim)
        widened = jnp.concatenate(
            [v_ref[:, lanes], jnp.ones((length, dim), jnp.bfloat16)], axis=1
        )
        for first in range(0, length, block):
            end = first + block
            scores = matmul_nt(q_ref[first:end, lanes], k_ref[:end, lanes])
            gap = level[h : h + 1, :end] - top_columns[first:end, h : h + 1]
            t = lax.broadcasted_iota(jnp.int32, (block, end), 0) + first
            s = lax.broadcasted_iota(jnp.int32, (block, end), 1)
            scores = scores * jnp.exp(jnp.where(s <= t, gap, lowest))
            coarse, fine = narrow(scores)
            pairs[h, first:end] = matmul(coarse, widened[:end]) + matmul(fine, widened[:end])

    chosen, share = slot_tables(ids_ref[...], wts_ref[...], experts, capacity, padded)
    share_ref[...] = share.reshape(experts, padded, rows)
    loads[2].wait()

    for k in evens:
        tiny_copy(k).wait_recv()
        tiny_copy(k + 1).start()
        mat_copy(k).wait_recv()
        mat_copy(k + 1).start()
    for k in [1] + [k + 1 for k in evens]:
        tiny_copy(k).wait_recv()
        mat_copy(k).wait_recv()

    decay = jnp.zeros((heads, dim), jnp.float32)
    levels, flags = [None] * n, [None] * n
    for s in reversed(range(n)):
        flags[s] = jnp.where(s < sp, 1.0, 0.0)
        levels[s] = flags[s] * (tiny[s, 2 * heads : 3 * heads] + decay) + (1.0 - flags[s]) * lowest
        decay = decay + flags[s] * tiny[s, heads : 2 * heads]
    prior_top = functools.reduce(jnp.maximum, levels)
    scales = [jnp.exp(levels[s] - prior_top) * flags[s] for s in range(n)]
    prior_norm = sum(scales[s] * tiny[s, :heads] for s in range(n))
    norm_columns = jnp.transpose(stack_rows([prior_norm], dim))
    reach = jnp.broadcast_to(prior_top[:, :1], (heads, length))
    joined = jnp.maximum(top, reach)
    factors = jnp.transpose(
        stack_rows(
            [
                jnp.exp(top - joined),
                jnp.exp(reach - joined),
                jnp.exp(-(total + joined)) * dim**0.5,
            ],
            length,
        )
    )
    for h in range(heads):
        lanes = slice(h * dim, (h + 1) * dim)
        prior = sum(
            scales[s][h : h + 1] * mats[s, lanes, :].astype(jnp.float32) for s in range(n)
        )
        prior = jnp.concatenate(
            [prior, jnp.broadcast_to(norm_columns[:, h : h + 1], (dim, dim))], axis=1
        )
        coarse, fine = narrow(prior)
        carried = matmul(q_ref[:, lanes], coarse) + matmul(q_ref[:, lanes], fine)
        both = pairs[h] * factors[:, h : h + 1]
        both = both + carried * factors[:, heads + h : heads + h + 1]
        guard = jnp.maximum(
            jnp.abs(both[:, dim:]), factors[:, 2 * heads + h : 2 * heads + h + 1]
        )
        hid[:, lanes] = (both[:, :dim] / guard).astype(jnp.bfloat16)

    group = max(1, 256 // columns)
    chunk = group * columns
    count = width // chunk

    def pass_on(k):
        piece_copy(k).wait_recv()
        piece_copy(k + 1).start()

    def near_far(i):
        return remote(
            partial.at[i, (p + 2) % 4], near.at[0, i], near_s.at[0, i], near_r.at[0, i], (sp, p)
        )

    def near_own(i):
        return remote(partial.at[i, p], near.at[1, i], near_s.at[1, i], near_r.at[1, i], (sp, p))

    def crossing(i):
        return remote(sent.at[i], far.at[i], far_s.at[i], far_r.at[i], (sp, q))

    def cross(i):
        near_far(i).wait_recv()
        both = partial[i, q].astype(jnp.float32) + near[0, i].astype(jnp.float32)
        sent[i] = both.astype(jnp.bfloat16)
        crossing(i).start()

    if group == 1:
        order = [0, 1] + evens + [k + 1 for k in evens]
        spots = [at(k) for k in order]
    else:
        order = spots = list(range(count))
        for k in evens:
            pass_on(k)
        for k in [1] + [k + 1 for k in evens]:
            piece_copy(k).wait_recv()
    for i, k in enumerate(order):
        if group > 1:
            piece = jnp.concatenate([pieces[i * group + j] for j in range(group)], axis=1)
        else:
            if k % 2:
                piece_copy(k).wait_recv()
            elif k:
                pass_on(k)
            piece = pieces[spots[i]]
        made = matmul(hid[...], piece).astype(jnp.bfloat16)
        partial[i] = made.reshape(length // rows, rows, chunk)
        near_far(i).start()
        near_own(i).start()
        if i:
            cross(i - 1)
    cross(count - 1)

    squares = jnp.zeros((rows, 1), jnp.float32)
    for i in range(count):
        near_own(i).wait_recv()
        crossing(i).wait_recv()
        where = pl.ds(pl.multiple_of(spots[i] * chunk, chunk), chunk)
        both = partial[i, tp].astype(jnp.float32) + near[1, i].astype(jnp.float32)
        both = both + far[i].astype(jnp.float32)
        mixed = (res_ref[:, where].astype(jnp.float32) + both).astype(jnp.bfloat16)
        mixed_ref[:, where] = mixed
        wide = mixed.astype(jnp.float32)
        squares = squares + jnp.sum(wide * wide, axis=1, keepdims=True)
    scale = lax.rsqrt(squares / width + epsilon)
    span = min(width, 512)
    for first in range(0, width, span):
        wide = mixed_ref[:, first : first + span].astype(jnp.float32)
        normed = (wide * scale * gain_ref[:, first : first + span]).astype(jnp.bfloat16)
        picked = matmul(chosen, normed).astype(jnp.bfloat16)
        x_ref[:, :, first : first + span] = picked.reshape(experts, padded, span)


    inner = ((sp // 2 + 1) // 2) % 2

    def pick(i, outer_order, inner_order):
        if n != 8:
            return (i + 1) % n
        return sum(
            jnp.where(i == j, a + inner * (b - a), 0)
            for j, (a, b) in enumerate(zip(outer_order, inner_order))
        )

    def turn(i):
        return pick(i, (1, 2, 3, 6, 7, 4, 5, 0), (1, 2, 4, 5, 3, 6, 7, 0))

    def home_turn(i):
        return pick(i, (1, 2, 4, 5, 6, 7, 3), (1, 2, 3, 4, 6, 5, 7))

    def direct(k):
        other = flip(sp, k, bits)
        return remote(
            x_ref.at[other], arrive.at[sp, tp], direct_s.at[k], direct_r.at[k], (other, tp)
        )

    def across(k, src):
        s = flip(sp, k, bits)
        return remote(src(s), arrive.at[s, tp], across_s.at[k], across_r.at[k], (sp, q))

    def side(k, src):
        s = flip(sp, k, bits)
        return remote(src(s), arrive.at[s, tp], side_s.at[k], side_r.at[k], (sp, p))

    def landed(s):
        return arrive.at[s, tp]

    def fresh(s):
        return x_ref.at[s]

    def relay(k):
        s = flip(sp, k, bits)
        return remote(
            arrive.at[s, q], arrive.at[s, q], relay_s.at[k], relay_r.at[k], (sp, p)
        )

    def close_far(k):
        s = flip(sp, k, bits)
        return remote(
            part.at[s, (p + 2) % 4], close.at[0, k], close_s.at[0, k], close_r.at[0, k], (sp, p)
        )

    def close_own(k):
        s = flip(sp, k, bits)
        return remote(part.at[s, p], close.at[1, k], close_s.at[1, k], close_r.at[1, k], (sp, p))

    def paying(k):
        return remote(paid.at[k], other_half.at[k], paid_s.at[k], paid_r.at[k], (sp, q))

    def homeward(k):
        other = flip(sp, k, bits)
        return remote(result.at[k], home.at[sp], home_s.at[k], home_r.at[k], (other, tp))

    for k in (1, 2, 4, 5, 6, 7, 3) if n == 8 else range(1, n):
        direct(k).start()
    across(0, fresh).start()
    side(0, fresh).start()
    arrive[sp, tp] = x_ref[sp]
    routed[...] = mixed_ref[...].astype(jnp.float32)
    for load in loads[3:]:
        load.wait()

    def merge(s, back):
        coarse, fine = narrow(share_ref[s])
        routed[...] += matmul_t(coarse, back) + matmul_t(fine, back)

    def fold(i):
        k = home_turn(i)
        homeward(k).wait_recv()
        s = flip(sp, k, bits)
        merge(s, home[s])

    early = min(3, n - 1)

    @pl.loop(0, n + 4)
    def _(i):
        @pl.when(i < n - 1)
        def _():
            k = turn(i)
            direct(k).wait_recv()
            across(k, landed).start()
            side(k, landed).start()

        @pl.when((i >= 1) & (i <= n))
        def _():
            k = turn(i - 1)
            across(k, landed).wait_recv()
            relay(k).start()

        @pl.when((i >= 2) & (i <= n + 1))
        def _():
            k = turn(i - 2)
            s = flip(sp, k, bits)
            side(k, landed).wait_recv()
            relay(k).wait_recv()
            pre = matmul(arrive[s].reshape(4 * padded, width), gate_up[...])
            gate = pre[:, :hidden]
            act = (gate / (1.0 + jnp.exp(-gate)) * pre[:, hidden:]).astype(jnp.bfloat16)
            out = matmul(act, down[...])
            part[s] = out.astype(jnp.bfloat16).reshape(4, padded, width)
            close_far(k).start()
            close_own(k).start()

        @pl.when((i >= 3) & (i <= n + 2))
        def _():
            k = turn(i - 3)
            s = flip(sp, k, bits)
            close_far(k).wait_recv()
            both = part[s, q].astype(jnp.float32) + close[0, k].astype(jnp.float32)
            paid[k] = both.astype(jnp.bfloat16)
            paying(k).start()

        @pl.when(i >= 4)
        def _():
            k = turn(i - 4)
            s = flip(sp, k, bits)
            close_own(k).wait_recv()
            paying(k).wait_recv()
            both = part[s, tp].astype(jnp.float32) + close[1, k].astype(jnp.float32)
            result[k] = (both + other_half[k].astype(jnp.float32)).astype(jnp.bfloat16)

            @pl.when(i < n + 3)
            def _():
                homeward(k).start()

        @pl.when((i >= 6) & (i < 6 + early))
        def _():
            fold(i - 6)

    merge(sp, result[0])

    @pl.loop(early, n - 1)
    def _(i):
        fold(i)

    out_ref[...] = routed[...].astype(jnp.bfloat16)

    @pl.loop(0, n)
    def _(k):
        @pl.when(k > 0)
        def _():
            homeward(k).wait_send()
            direct(k).wait_send()

        across(k, landed).wait_send()
        side(k, landed).wait_send()
        relay(k).wait_send()
        close_far(k).wait_send()
        close_own(k).wait_send()
        paying(k).wait_send()

    for k in range(1, n):
        tiny_copy(k).wait_send()
        mat_copy(k).wait_send()
        piece_copy(k).wait_send()
    for i in range(count):
        near_far(i).wait_send()
        near_own(i).wait_send()
        crossing(i).wait_send()


def layer(capacity, q, k, v, gate_in, forget, extra, residual, weight, gain, ids, wts, *mats):
    n = lax.axis_size("sp")
    length, channels = q.shape
    heads = gate_in.shape[0]
    dim = channels // heads
    rows, width = residual.shape
    columns = weight.shape[1]
    chunk = max(1, 256 // columns) * columns
    count = width // chunk
    padded = -(-capacity // 8) * 8
    hidden = mats[2].shape[1]
    vmem = pl.BlockSpec(memory_space=pltpu.VMEM)
    hbm = pl.BlockSpec(memory_space=pl.ANY)
    dma = pltpu.SemaphoreType.DMA
    kind = residual.dtype
    block = (n, padded, width)
    shapes = [
        (length, channels), (rows, width), (channels, dim), (n, channels, dim), None, None,
        (n, channels, columns), None, (length, channels), (count, length // rows, rows, chunk),
        (2, count, rows, chunk), (count, rows, chunk), (count, rows, chunk),
        block, (rows, width), None, (width, 2 * hidden), (hidden, width),
        (n, 4) + block[1:], (n, 4) + block[1:], (2,) + block, block, block, block, block, None,
    ]
    wide = iter(
        [(8, dim), (n, 8, dim), (heads, length, 2 * dim), (n, padded, rows), (rows, width)]
    )
    return pl.pallas_call(
        functools.partial(layer_kernel, capacity, padded),
        out_shape=jax.ShapeDtypeStruct((rows, width), kind),
        in_specs=[hbm] + [vmem] * 5 + [hbm] * 2 + [vmem] * 3 + [hbm] * 3,
        out_specs=vmem,
        scratch_shapes=[
            pltpu.VMEM(shape, kind) if shape else pltpu.VMEM(next(wide), jnp.float32)
            for shape in shapes
        ]
        + [dma((6,))]
        + [dma((n,))] * 6
        + [dma((2, count))] * 2
        + [dma((count,))] * 2
        + [dma((n,))] * 8
        + [dma((2, n))] * 2
        + [dma((n,))] * 4,
        compiler_params=pltpu.CompilerParams(
            collective_id=1, has_side_effects=True, vmem_limit_bytes=61 * 2**20
        ),
    )(q, k, v, gate_in, forget, extra, residual, weight, gain, ids, wts, *mats)


def local(
    memory_queries,
    memory_keys,
    memory_values,
    input_gate_logits,
    forget_gate_logits,
    extra_log_decay,
    residual,
    cell_output_weight,
    expert_norm_gain,
    expert_gate_weight,
    expert_up_weight,
    expert_down_weight,
    routed_expert_index,
    routed_expert_weight,
):
    row_count = residual.shape[0]
    experts = lax.axis_size("sp") * expert_gate_weight.shape[0]
    assigned = row_count * routed_expert_index.shape[1]
    capacity = max(2, assigned * 5 // (4 * experts))
    own_ids = lax.dynamic_slice_in_dim(
        routed_expert_index, lax.axis_index("tp") * row_count, row_count, 0
    )
    return layer(
        capacity,
        memory_queries,
        memory_keys,
        memory_values,
        input_gate_logits,
        forget_gate_logits,
        extra_log_decay,
        residual,
        cell_output_weight,
        expert_norm_gain[None, :],
        own_ids.T,
        routed_expert_weight.T,
        expert_gate_weight,
        expert_up_weight,
        expert_down_weight,
    )


def solution(mesh):
    return jax.shard_map(
        local,
        mesh=mesh,
        in_specs=(
            P("sp", "tp"),
            P("sp", "tp"),
            P("sp", "tp"),
            P("tp", "sp"),
            P("tp", "sp"),
            P("tp", "sp"),
            P(("sp", "tp"), None),
            P("tp", "sp"),
            P(),
            P("sp", None, "tp"),
            P("sp", None, "tp"),
            P("sp", "tp", None),
            P("sp", None),
            P(("sp", "tp"), None),
        ),
        out_specs=P(("sp", "tp"), None),
        check_vma=False,
    )
```

```python
import functools
import jax
import jax.numpy as jnp
from jax import lax
from jax.experimental import pallas as pl
from jax.experimental.pallas import tpu as pltpu
from jax.sharding import PartitionSpec as P

highest = lax.Precision.HIGHEST
lowest = -1e30
epsilon = 1e-06


def places():
    sp, tp = lax.axis_index("sp"), lax.axis_index("tp")
    n = lax.axis_size("sp")
    return sp, tp, n, tp + 1 - 2 * (tp % 2), (tp + 2) % 4


def announce(devices):
    barrier = pltpu.get_barrier_semaphore()
    for device in devices:
        pl.semaphore_signal(
            barrier, inc=1, device_id=device, device_id_type=pl.DeviceIdType.MESH
        )
    return len(devices)


def remote(src, dst, send, recv, device):
    return pltpu.make_async_remote_copy(
        src_ref=src,
        dst_ref=dst,
        send_sem=send,
        recv_sem=recv,
        device_id=device,
        device_id_type=pl.DeviceIdType.MESH,
    )


def flip(place, k, bits):
    out = place
    for b in range(bits):
        step = 1 << b
        out = out + ((k // step) % 2) * step * (1 - 2 * ((place // step) % 2))
    return out


def narrow(x):
    coarse = x.astype(jnp.bfloat16)
    return coarse, (x - coarse.astype(jnp.float32)).astype(jnp.bfloat16)


def matmul(a, b):
    return jnp.dot(a, b, preferred_element_type=jnp.float32)


def matmul_t(a, b):
    return lax.dot_general(a, b, (((0,), (0,)), ((), ())), preferred_element_type=jnp.float32)


def matmul_nt(a, b):
    return lax.dot_general(a, b, (((1,), (1,)), ((), ())), preferred_element_type=jnp.float32)


def stack_rows(pieces, length):
    used = sum(piece.shape[0] for piece in pieces)
    return jnp.concatenate(list(pieces) + [jnp.zeros((-used % 8, length), jnp.float32)], axis=0)


def running_sum(x):
    rows, length = x.shape
    parts, rest = [], x
    for _ in range(3):
        part = rest.astype(jnp.bfloat16).astype(jnp.float32)
        parts.append(part)
        rest = rest - part
    stacked = stack_rows(parts, length).astype(jnp.bfloat16)
    at = lax.broadcasted_iota(jnp.int32, (length, length), 0)
    to = lax.broadcasted_iota(jnp.int32, (length, length), 1)
    sums = matmul(stacked, jnp.where(at <= to, 1.0, 0.0).astype(jnp.bfloat16))
    return sums[:rows] + sums[rows : 2 * rows] + sums[2 * rows : 3 * rows]


def running_max(x):
    length = x.shape[1]
    lane = lax.broadcasted_iota(jnp.int32, x.shape, 1)
    step = 1
    while step < length:
        x = jnp.maximum(x, jnp.where(lane >= step, pltpu.roll(x, step, 1), lowest))
        step *= 2
    return x


def slot_tables(ids, weights, experts, capacity, padded):
    rows = ids.shape[1]
    names = lax.broadcasted_iota(jnp.int32, (experts, rows), 0)
    hits = [ids[j : j + 1] == names for j in range(ids.shape[0])]
    named = sum(jnp.where(hit, 1.0, 0.0) for hit in hits)
    at = lax.broadcasted_iota(jnp.int32, (rows, rows), 0)
    to = lax.broadcasted_iota(jnp.int32, (rows, rows), 1)
    before = matmul(named.astype(jnp.bfloat16), jnp.where(at < to, 1.0, 0.0).astype(jnp.bfloat16))
    slot = lax.broadcasted_iota(jnp.int32, (experts * padded, rows), 0)
    chosen, share = 0.0, 0.0
    for j, hit in enumerate(hits):
        rank = jnp.sum(jnp.where(hit, before, 0.0), axis=0, keepdims=True)
        here = (ids[j : j + 1] * padded + rank.astype(jnp.int32)) == slot
        chosen = chosen + jnp.where(here, 1.0, 0.0)
        share = share + jnp.where(here, weights[j : j + 1], 0.0)
    return chosen.astype(jnp.bfloat16), share


def layer_kernel(
    capacity, padded,
    q_hbm, k_hbm, v_hbm, in_hbm, forget_hbm, extra_hbm, res_hbm, w_hbm, gain_hbm, ids_hbm, wts_hbm,
    gate_hbm, up_hbm, down_hbm, out_ref,
    k_ref, v_ref, in_ref, forget_ref, extra_ref, gain_ref, ids_ref, wts_ref, q_ref, res_ref, mine, mats, tiny_mine, tiny, pieces, pairs, hid, partial, near, sent, far,
    x_ref, mixed_ref, share_ref, gate_up, down, arrive, part, close, paid, other_half, result,
    home, routed,
    load_sems, early_sems, mat_s, mat_r, tiny_s, tiny_r, piece_s, piece_r, near_s, near_r, far_s, far_r,
    direct_s, direct_r, across_s, across_r, side_s, side_r, relay_s, relay_r,
    close_s, close_r, paid_s, paid_r, home_s, home_r,
):
    sp, tp, n, p, q = places()
    bits = n.bit_length() - 1
    length, channels = k_ref.shape
    heads = in_ref.shape[0]
    dim = channels // heads
    rows, width = out_ref.shape
    columns = pieces.shape[2]
    hidden = down.shape[0]
    experts = n
    group = max(1, 256 // columns)
    chunk = group * columns
    count = width // chunk
    count_greeted = announce([(flip(sp, k, bits), tp) for k in range(1, n)] + [(sp, p), (sp, q)])
    loads = [
        pltpu.make_async_copy(w_hbm, pieces.at[sp], load_sems.at[0]),
        pltpu.make_async_copy(q_hbm, q_ref, load_sems.at[1]),
        pltpu.make_async_copy(res_hbm, res_ref, load_sems.at[2]),
        pltpu.make_async_copy(gate_hbm.at[0], gate_up.at[:, pl.ds(0, hidden)], load_sems.at[3]),
        pltpu.make_async_copy(up_hbm.at[0], gate_up.at[:, pl.ds(hidden, hidden)], load_sems.at[4]),
        pltpu.make_async_copy(down_hbm.at[0], down, load_sems.at[5]),
    ]
    early_loads = [
        pltpu.make_async_copy(src, dst, early_sems.at[j])
        for j, (src, dst) in enumerate(
            [
                (forget_hbm, forget_ref), (extra_hbm, extra_ref), (in_hbm, in_ref),
                (k_hbm, k_ref), (v_hbm, v_ref),
                (ids_hbm, ids_ref), (wts_hbm, wts_ref), (gain_hbm, gain_ref),
            ]
        )
    ]
    for load in early_loads + loads[:3]:
        load.start()
    for load in early_loads:
        load.wait()
    evens = list(range(2, n, 2))

    def at(k):
        return flip(sp, k, bits)

    def mat_copy(k):
        src = mine if k < 2 else (mine if k % 2 == 0 else mats.at[at(k - 1)])
        slot = sp if k % 2 == 0 or k == 1 else at(k - 1)
        to = at(1) if k % 2 else at(k)
        return remote(src, mats.at[slot], mat_s.at[k], mat_r.at[k], (to, tp))

    def tiny_copy(k):
        src = tiny_mine if k % 2 == 0 or k == 1 else tiny.at[at(k - 1)]
        slot = sp if k % 2 == 0 or k == 1 else at(k - 1)
        to = at(1) if k % 2 else at(k)
        return remote(src, tiny.at[slot], tiny_s.at[k], tiny_r.at[k], (to, tp))

    def piece_copy(k):
        slot = sp if k % 2 == 0 or k == 1 else at(k - 1)
        src = pieces.at[slot]
        to = at(1) if k % 2 else at(k)
        return remote(src, pieces.at[slot], piece_s.at[k], piece_r.at[k], (to, tp))

    def pass_on(k):
        piece_copy(k).wait_recv()
        piece_copy(k + 1).start()

    logits = forget_ref[...]
    log_forget = (
        jnp.minimum(logits, 0.0) - jnp.log1p(jnp.exp(-jnp.abs(logits))) + extra_ref[...]
    )
    total = running_sum(log_forget)
    level = in_ref[...] - total
    peak = jnp.max(level, axis=1, keepdims=True)
    retain = jnp.exp(level - peak)
    retain_columns = jnp.transpose(stack_rows([retain], length))
    for h in range(heads):
        lanes = slice(h * dim, (h + 1) * dim)
        kept = narrow(v_ref[:, lanes].astype(jnp.float32) * retain_columns[:, h : h + 1])
        mat = matmul_t(k_ref[:, lanes], kept[0]) + matmul_t(k_ref[:, lanes], kept[1])
        mine[lanes, :] = mat.astype(jnp.bfloat16)
    coarse, fine = narrow(retain)
    sums = matmul(
        stack_rows([coarse.astype(jnp.float32), fine.astype(jnp.float32)], length).astype(jnp.bfloat16),
        k_ref[...],
    )
    norms = [
        sums[h : h + 1, h * dim : (h + 1) * dim]
        + sums[heads + h : heads + h + 1, h * dim : (h + 1) * dim]
        for h in range(heads)
    ]
    last = total[:, length - 1 : length]
    tiny_mine[...] = stack_rows(
        norms + [jnp.broadcast_to(last, (heads, dim)), jnp.broadcast_to(last + peak, (heads, dim))], dim
    )
    pl.semaphore_wait(pltpu.get_barrier_semaphore(), count_greeted)
    for k in evens + [1]:
        tiny_copy(k).start()
        mat_copy(k).start()
    loads[0].wait()
    for k in [1] + evens:
        piece_copy(k).start()
    for load in loads[3:]:
        load.start()
    mats[sp] = mine[...]
    tiny[sp] = tiny_mine[...]
    loads[1].wait()

    top = running_max(level)
    top_columns = jnp.transpose(stack_rows([top], length))
    block = min(length, 256)
    for h in range(heads):
        lanes = slice(h * dim, (h + 1) * dim)
        widened = jnp.concatenate(
            [v_ref[:, lanes], jnp.ones((length, dim), jnp.bfloat16)], axis=1
        )
        for first in range(0, length, block):
            end = first + block
            scores = matmul_nt(q_ref[first:end, lanes], k_ref[:end, lanes])
            gap = level[h : h + 1, :end] - top_columns[first:end, h : h + 1]
            t = lax.broadcasted_iota(jnp.int32, (block, end), 0) + first
            s = lax.broadcasted_iota(jnp.int32, (block, end), 1)
            scores = scores * jnp.exp(jnp.where(s <= t, gap, lowest))
            coarse, fine = narrow(scores)
            pairs[h, first:end] = matmul(coarse, widened[:end]) + matmul(fine, widened[:end])

    ids = ids_ref[:, pl.ds(pl.multiple_of(tp * rows, rows), rows)]
    chosen, share = slot_tables(ids, wts_ref[...], experts, capacity, padded)
    share_ref[...] = share.reshape(experts, padded, rows)
    loads[2].wait()

    for k in evens:
        tiny_copy(k).wait_recv()
        tiny_copy(k + 1).start()
        mat_copy(k).wait_recv()
        mat_copy(k + 1).start()
    if group == 1:
        pass_on(2)
    for k in [1] + [k + 1 for k in evens]:
        tiny_copy(k).wait_recv()
        mat_copy(k).wait_recv()

    decay = jnp.zeros((heads, dim), jnp.float32)
    levels, flags = [None] * n, [None] * n
    for s in reversed(range(n)):
        flags[s] = jnp.where(s < sp, 1.0, 0.0)
        levels[s] = flags[s] * (tiny[s, 2 * heads : 3 * heads] + decay) + (1.0 - flags[s]) * lowest
        decay = decay + flags[s] * tiny[s, heads : 2 * heads]
    prior_top = functools.reduce(jnp.maximum, levels)
    scales = [jnp.exp(levels[s] - prior_top) * flags[s] for s in range(n)]
    prior_norm = sum(scales[s] * tiny[s, :heads] for s in range(n))
    norm_columns = jnp.transpose(stack_rows([prior_norm], dim))
    reach = jnp.broadcast_to(prior_top[:, :1], (heads, length))
    joined = jnp.maximum(top, reach)
    factors = jnp.transpose(
        stack_rows(
            [
                jnp.exp(top - joined),
                jnp.exp(reach - joined),
                jnp.exp(-(total + joined)) * dim**0.5,
            ],
            length,
        )
    )
    for h in range(heads):
        lanes = slice(h * dim, (h + 1) * dim)
        prior = sum(
            scales[s][h : h + 1] * mats[s, lanes, :].astype(jnp.float32) for s in range(n)
        )
        prior = jnp.concatenate(
            [prior, jnp.broadcast_to(norm_columns[:, h : h + 1], (dim, dim))], axis=1
        )
        coarse, fine = narrow(prior)
        carried = matmul(q_ref[:, lanes], coarse) + matmul(q_ref[:, lanes], fine)
        both = pairs[h] * factors[:, h : h + 1]
        both = both + carried * factors[:, heads + h : heads + h + 1]
        guard = jnp.maximum(
            jnp.abs(both[:, dim:]), factors[:, 2 * heads + h : 2 * heads + h + 1]
        )
        hid[:, lanes] = (both[:, :dim] / guard).astype(jnp.bfloat16)

    def near_far(i):
        return remote(
            partial.at[i, (p + 2) % 4], near.at[0, i], near_s.at[0, i], near_r.at[0, i], (sp, p)
        )

    def near_own(i):
        return remote(partial.at[i, p], near.at[1, i], near_s.at[1, i], near_r.at[1, i], (sp, p))

    def crossing(i):
        return remote(sent.at[i], far.at[i], far_s.at[i], far_r.at[i], (sp, q))

    def cross(i):
        near_far(i).wait_recv()
        both = partial[i, q].astype(jnp.float32) + near[0, i].astype(jnp.float32)
        sent[i] = both.astype(jnp.bfloat16)
        crossing(i).start()

    inner = ((sp // 2 + 1) // 2) % 2

    def pick(i, outer_order, inner_order):
        if n != 8:
            return (i + 1) % n
        return sum(
            jnp.where(i == j, a + inner * (b - a), 0)
            for j, (a, b) in enumerate(zip(outer_order, inner_order))
        )

    def turn(i):
        return pick(i, (1, 2, 3, 6, 7, 4, 5, 0), (1, 2, 4, 5, 3, 6, 7, 0))

    def home_turn(i):
        return pick(i, (1, 2, 4, 5, 6, 7, 3), (1, 2, 3, 4, 6, 5, 7))

    def span(s, h):
        first = s // (n // 2) if group == 1 else 0
        return pl.ds(pl.multiple_of((first + h) % 2 * (width // 2), width // 2), width // 2)

    def landed(s, h):
        return arrive.at[s, tp, :, span(s, h)]

    def fresh(s, h):
        return x_ref.at[s, :, span(s, h)]

    def direct(k, h):
        other = flip(sp, k, bits)
        return remote(
            x_ref.at[other, :, span(sp, h)], landed(sp, h),
            direct_s.at[h, k], direct_r.at[h, k], (other, tp),
        )

    def across(k, h, src=landed):
        s = flip(sp, k, bits)
        return remote(src(s, h), landed(s, h), across_s.at[h, k], across_r.at[h, k], (sp, q))

    def side(k, h, src=landed):
        s = flip(sp, k, bits)
        return remote(src(s, h), landed(s, h), side_s.at[h, k], side_r.at[h, k], (sp, p))

    def relay(k, h):
        s = flip(sp, k, bits)
        block = arrive.at[s, q, :, span(s, h)]
        return remote(block, block, relay_s.at[h, k], relay_r.at[h, k], (sp, p))

    def take(i, h):
        k = turn(i)
        direct(k, h).wait_recv()
        across(k, h).start()
        side(k, h).start()

    def finish(i):
        near_own(i).wait_recv()
        crossing(i).wait_recv()
        where = pl.ds(pl.multiple_of(spots[i] * chunk, chunk), chunk)
        both = partial[i, tp].astype(jnp.float32) + near[1, i].astype(jnp.float32)
        both = both + far[i].astype(jnp.float32)
        mixed = res_ref[:, where].astype(jnp.float32) + both
        mixed_ref[:, where] = mixed.astype(jnp.bfloat16)

    def publish(h):
        where = span(sp, h)
        picked = matmul(chosen, mixed_ref[:, where]).astype(jnp.bfloat16)
        x_ref[:, :, where] = picked.reshape(experts, padded, width // 2)
        for k in (1, 2, 4, 5, 6, 7, 3) if n == 8 else range(1, n):
            direct(k, h).start()
        across(0, h, fresh).start()
        side(0, h, fresh).start()


    if group == 1:
        order = [0, 1] + evens[:1] + [3] + evens[1:] + [k + 1 for k in evens[1:]]
        spots = [at(k) for k in order]
    else:
        order = spots = list(range(count))
        for k in evens:
            pass_on(k)
        for k in [1] + [k + 1 for k in evens]:
            piece_copy(k).wait_recv()
    for i, k in enumerate(order):
        if i == 3 and group == 1:
            for even in evens[1:]:
                pass_on(even)
        if group > 1:
            piece = jnp.concatenate([pieces[i * group + j] for j in range(group)], axis=1)
        else:
            if k % 2:
                piece_copy(k).wait_recv()
            piece = pieces[spots[i]]
        made = matmul(hid[...], piece).astype(jnp.bfloat16)
        partial[i] = made.reshape(length // rows, rows, chunk)
        near_far(i).start()
        near_own(i).start()
        if i:
            cross(i - 1)
        if i == count // 2:
            for j in range(i):
                finish(j)
            publish(0)
    cross(count - 1)
    for j in range(count // 2, count):
        finish(j)
        if j == count - 4:
            take(0, 0)
        if j == count - 2:
            take(1, 0)
    publish(1)
    lead = 4
    take(2, 0)
    take(3, 0)

    def close_far(k):
        s = flip(sp, k, bits)
        return remote(
            part.at[s, (p + 2) % 4], close.at[0, k], close_s.at[0, k], close_r.at[0, k], (sp, p)
        )

    def close_own(k):
        s = flip(sp, k, bits)
        return remote(part.at[s, p], close.at[1, k], close_s.at[1, k], close_r.at[1, k], (sp, p))

    def paying(k):
        return remote(paid.at[k], other_half.at[k], paid_s.at[k], paid_r.at[k], (sp, q))

    def homeward(k):
        other = flip(sp, k, bits)
        return remote(result.at[k], home.at[sp], home_s.at[k], home_r.at[k], (other, tp))

    arrive[sp, tp] = x_ref[sp]
    routed[...] = mixed_ref[...].astype(jnp.float32)
    for load in loads[3:]:
        load.wait()

    def merge(s, back):
        coarse, fine = narrow(share_ref[s])
        routed[...] += matmul_t(coarse, back) + matmul_t(fine, back)

    def fold(i):
        k = home_turn(i)
        homeward(k).wait_recv()
        s = flip(sp, k, bits)
        merge(s, home[s])

    early = min(3, n - 1)

    @pl.loop(0, n + 4)
    def _(i):
        @pl.when(i < n - 1)
        def _():
            take(i, 1)

        @pl.when(i < n - 1 - lead)
        def _():
            take(i + lead, 0)

        @pl.when((i >= 1) & (i <= n))
        def _():
            k = turn(i - 1)
            for h in range(2):
                across(k, h).wait_recv()
                relay(k, h).start()

        @pl.when((i >= 2) & (i <= n + 1))
        def _():
            k = turn(i - 2)
            s = flip(sp, k, bits)
            for h in range(2):
                side(k, h).wait_recv()
                relay(k, h).wait_recv()
            wide = arrive[s].reshape(4 * padded, width).astype(jnp.float32)
            scale = lax.rsqrt(jnp.mean(wide * wide, axis=1, keepdims=True) + epsilon)
            pre = matmul((wide * scale * gain_ref[...]).astype(jnp.bfloat16), gate_up[...])
            gate = pre[:, :hidden]
            act = (gate / (1.0 + jnp.exp(-gate)) * pre[:, hidden:]).astype(jnp.bfloat16)
            out = matmul(act, down[...])
            part[s] = out.astype(jnp.bfloat16).reshape(4, padded, width)
            close_far(k).start()
            close_own(k).start()

        @pl.when((i >= 3) & (i <= n + 2))
        def _():
            k = turn(i - 3)
            s = flip(sp, k, bits)
            close_far(k).wait_recv()
            both = part[s, q].astype(jnp.float32) + close[0, k].astype(jnp.float32)
            paid[k] = both.astype(jnp.bfloat16)
            paying(k).start()

        @pl.when(i == n + 3)
        def _():
            for f in range(early, min(early + 2, n - 1)):
                fold(f)

        @pl.when(i >= 4)
        def _():
            k = turn(i - 4)
            s = flip(sp, k, bits)
            close_own(k).wait_recv()
            paying(k).wait_recv()
            both = part[s, tp].astype(jnp.float32) + close[1, k].astype(jnp.float32)
            result[k] = (both + other_half[k].astype(jnp.float32)).astype(jnp.bfloat16)

            @pl.when(i < n + 3)
            def _():
                homeward(k).start()

        @pl.when((i >= 6) & (i < 6 + early))
        def _():
            fold(i - 6)

    merge(sp, result[0])

    @pl.loop(min(early + 2, n - 1), n - 1)
    def _(i):
        fold(i)

    out_ref[...] = routed[...].astype(jnp.bfloat16)

    @pl.loop(0, n)
    def _(k):
        @pl.when(k > 0)
        def _():
            homeward(k).wait_send()
            for h in range(2):
                direct(k, h).wait_send()

        for h in range(2):
            across(k, h).wait_send()
            side(k, h).wait_send()
            relay(k, h).wait_send()
        close_far(k).wait_send()
        close_own(k).wait_send()
        paying(k).wait_send()

    for k in range(1, n):
        tiny_copy(k).wait_send()
        mat_copy(k).wait_send()
        piece_copy(k).wait_send()
    for i in range(count):
        near_far(i).wait_send()
        near_own(i).wait_send()
        crossing(i).wait_send()


def layer(capacity, q, k, v, gate_in, forget, extra, residual, weight, gain, ids, wts, *mats):
    n = lax.axis_size("sp")
    length, channels = q.shape
    heads = gate_in.shape[0]
    dim = channels // heads
    rows, width = residual.shape
    columns = weight.shape[1]
    chunk = max(1, 256 // columns) * columns
    count = width // chunk
    padded = -(-capacity // 8) * 8
    hidden = mats[2].shape[1]
    vmem = pl.BlockSpec(memory_space=pltpu.VMEM)
    hbm = pl.BlockSpec(memory_space=pltpu.HBM)
    dma = pltpu.SemaphoreType.DMA
    kind = residual.dtype
    block = (n, padded, width)
    shapes = [
        (length, channels), (rows, width), (channels, dim), (n, channels, dim), None, None,
        (n, channels, columns), None, (length, channels), (count, length // rows, rows, chunk),
        (2, count, rows, chunk), (count, rows, chunk), (count, rows, chunk),
        block, (rows, width), None, (width, 2 * hidden), (hidden, width),
        (n, 4) + block[1:], (n, 4) + block[1:], (2,) + block, block, block, block, block, None,
    ]
    wide = iter(
        [(8, dim), (n, 8, dim), (heads, length, 2 * dim), (n, padded, rows), (rows, width)]
    )
    return pl.pallas_call(
        functools.partial(layer_kernel, capacity, padded),
        out_shape=jax.ShapeDtypeStruct((rows, width), kind),
        in_specs=[hbm] * 14,
        out_specs=vmem,
        scratch_shapes=[
            pltpu.VMEM(ref.shape, ref.dtype)
            for ref in (k, v, gate_in, forget, extra, gain, ids, wts)
        ]
        + [
            pltpu.VMEM(shape, kind) if shape else pltpu.VMEM(next(wide), jnp.float32)
            for shape in shapes
        ]
        + [dma((6,)), dma((8,))]
        + [dma((n,))] * 6
        + [dma((2, count))] * 2
        + [dma((count,))] * 2
        + [dma((2, n))] * 10
        + [dma((n,))] * 4,
        compiler_params=pltpu.CompilerParams(
            collective_id=1, has_side_effects=True, vmem_limit_bytes=61 * 2**20
        ),
    )(q, k, v, gate_in, forget, extra, residual, weight, gain, ids, wts, *mats)


def local(
    memory_queries,
    memory_keys,
    memory_values,
    input_gate_logits,
    forget_gate_logits,
    extra_log_decay,
    residual,
    cell_output_weight,
    expert_norm_gain,
    expert_gate_weight,
    expert_up_weight,
    expert_down_weight,
    routed_expert_index,
    routed_expert_weight,
):
    row_count = residual.shape[0]
    experts = lax.axis_size("sp") * expert_gate_weight.shape[0]
    assigned = row_count * routed_expert_index.shape[1]
    capacity = max(2, assigned * 5 // (4 * experts))
    return layer(
        capacity,
        memory_queries,
        memory_keys,
        memory_values,
        input_gate_logits,
        forget_gate_logits,
        extra_log_decay,
        residual,
        cell_output_weight,
        expert_norm_gain[None, :],
        routed_expert_index.T,
        routed_expert_weight.T,
        expert_gate_weight,
        expert_up_weight,
        expert_down_weight,
    )


def solution(mesh):
    return jax.shard_map(
        local,
        mesh=mesh,
        in_specs=(
            P("sp", "tp"),
            P("sp", "tp"),
            P("sp", "tp"),
            P("tp", "sp"),
            P("tp", "sp"),
            P("tp", "sp"),
            P(("sp", "tp"), None),
            P("tp", "sp"),
            P(),
            P("sp", None, "tp"),
            P("sp", None, "tp"),
            P("sp", "tp", None),
            P("sp", None),
            P(("sp", "tp"), None),
        ),
        out_specs=P(("sp", "tp"), None),
        check_vma=False,
    )
```
